32 devices in a mesh: ep: 4 (over y, x), tp: 8 (over z, core).
Axes of the slice: x: 2, y: 2, z: 4, core: 2. Of those that a mesh axis runs over, the one named last changes fastest.
Arguments:
- tokens: bfloat16 [64, 4096], P('ep'), may hold values from -6 to 6
- attn_gain: float32 [4096], replicated, may hold values from 0.1 to 1.9
- w_query: bfloat16 [4096, 2048], P('ep', 'tp'), may hold values from -0.15625 to 0.15625
- w_key: bfloat16 [4096, 2048], P('ep', 'tp'), may hold values from -0.09375 to 0.09375
- w_value: bfloat16 [4096, 2048], P('ep', 'tp'), may hold values from -0.09375 to 0.09375
- mix_lambda: float32 [16], P('tp'), may hold values from 0.3 to 0.8
- head_gain: float32 [128], replicated, may hold values from 0.1 to 1.9
- w_output: bfloat16 [2048, 4096], P('tp'), may hold values from -0.125 to 0.125
- cache_keys: bfloat16 [64, 1024, 2048], P('ep', None, 'tp'), may hold values from -180 to 180
- cache_value: bfloat16 [64, 1024, 2048], P('ep', None, 'tp'), may hold values from -6 to 6
- lengths: int32 [64], P('ep'), may hold values from 1 to 1024
- moe_gain: float32 [4096], replicated, may hold values from 0.1 to 1.9
- group_ids: int32 [64], P('ep'), may hold values from 0 to 1, as said below
- member_ids: int32 [64, 2], P('ep'), may hold values from 0 to 1, as said below
- group_gate: float32 [64], P('ep'), may hold values from 0.3 to 1
- member_logits: float32 [64, 2], P('ep'), may hold values from -4 to 4
- w_exp_gate: bfloat16 [4, 4096, 2048], P('ep', None, 'tp'), may hold values from -0.09375 to 0.09375
- w_exp_up: bfloat16 [4, 4096, 2048], P('ep', None, 'tp'), may hold values from -0.09375 to 0.09375
- w_exp_down: bfloat16 [4, 2048, 4096], P('ep', 'tp'), may hold values from -0.125 to 0.125
Outputs:
- mixed: bfloat16 [64, 4096], P('ep', 'tp')
- fresh_keys: bfloat16 [64, 2048], P('ep', 'tp')
- fresh_value: bfloat16 [64, 2048], P('ep', 'tp')
The draws below stay inside these ranges and needn't reach their ends.
Inputs may be any that keep to these rules, and one draw needn't show every extreme that they name: `group_ids`: each index of ep holds 16 consecutive tokens, of which every group gets the same number. A token's 2 members differ, and every expert group_ids * 2 + member_ids receives exactly 8 of the token-expert pairs of each index of ep.
All inputs are finite; a program needn't handle non-finite values.
Results may differ from the reference program's by a relative error of at most 0.015.
The reference program's roundings to bfloat16 on the way count: a program that leaves them out, or rounds other values in their place, can miss the bound.
Values may be sent and summed in bfloat16 or wider, within the bound.
A program may use at most 64 MiB of HBM per device.

```python
import jax
import jax.numpy as jnp
from jax import lax

D = 4096
HEADS = 16
DH = 64
FF = 2048
EPG = 2
TOPK = 2
SEQ_DEV = 16
CACHE = 1024
EXPERTS = 4
GROUPS = 2
BATCH = 64
N_EP = 4
N_TP = 8


def routing_tables(key):
    perm_key, start_key, shift_key = jax.random.split(jax.random.fold_in(key, 11), 3)
    perms = jax.vmap(lambda sub: jax.random.permutation(sub, SEQ_DEV))(jax.random.split(perm_key, N_EP))
    starts = jax.random.randint(start_key, (N_EP, GROUPS), 0, EPG)
    shifts = jax.random.randint(shift_key, (N_EP, GROUPS), 1, EPG)
    group = perms % GROUPS
    inside = perms // GROUPS
    start_row = jnp.take_along_axis(starts, group, axis=1)
    shift_row = jnp.take_along_axis(shifts, group, axis=1)
    first = (start_row + inside) % EPG
    second = (start_row + inside + shift_row) % EPG
    members = jnp.stack([first, second], axis=-1)
    return (group.reshape(BATCH).astype(jnp.int32), members.reshape(BATCH, TOPK).astype(jnp.int32))


def draw_group_ids(key, part):
    group, members = routing_tables(key)
    return group


def draw_member_ids(key, part):
    group, members = routing_tables(key)
    return members


def draw_cache_keys(key, part):
    base_key = jax.random.fold_in(jax.random.fold_in(key, 21), 0)
    base = jax.random.truncated_normal(base_key, -6.0, 6.0, (BATCH, CACHE, HEADS * 2 * DH), jnp.float32)
    return base.astype(jnp.bfloat16)


def touch_ends(entries, key, least, top_value):
    place = [jax.random.randint(jax.random.fold_in(key, axis), (), 0, length) for axis, length in enumerate(entries.shape)]
    main_axis = entries.shape.index(max(entries.shape))
    next_to = place[:main_axis] + [(place[main_axis] + 1) % entries.shape[main_axis]] + place[main_axis + 1:]
    return entries.at[tuple(place)].set(least).at[tuple(next_to)].set(top_value)


def block_levels(key, dims, cuts, smallest, largest):
    loudness, own = 1.0, jax.random.fold_in(key, 6)
    for dim, blocks in cuts:
        draws = jnp.exp(jax.random.uniform(jax.random.fold_in(own, dim), (blocks,), jnp.float32, smallest / len(cuts), largest / len(cuts)))
        loudness = loudness * jnp.repeat(draws, dims[dim] // blocks).reshape([-1 if axis == dim else 1 for axis in range(len(dims))])
    return loudness


def gaussian(rng, dims, width, most, shards=(), held_as=jnp.bfloat16):
    level = block_levels(rng, dims, shards, -0.22, 0.18) if shards else 1.0
    values = jax.random.normal(rng, dims, jnp.float32) * width * level
    return jnp.minimum(jnp.maximum(values, -most), most).astype(held_as)


def setup_inputs(seed: int = 0) -> dict:
    key_of = jax.random.split(jax.random.key(seed), 20)
    return {
        "tokens": gaussian(key_of[0], (BATCH, D), 1.0, 6.0, ((0, 4),)),
        "attn_gain": jnp.clip(1.0 + 0.18 * jax.random.normal(key_of[1], (D,), jnp.float32), 0.1, 1.9),
        "w_query": gaussian(key_of[2], (D, HEADS * 2 * DH), (D // 3) ** -0.5, 0.15625, ((0, 4), (1, 8))),
        "w_key": gaussian(key_of[3], (D, HEADS * 2 * DH), D ** -0.5, 0.09375, ((0, 4), (1, 8))),
        "w_value": gaussian(key_of[4], (D, HEADS * 2 * DH), D ** -0.5, 0.09375, ((0, 4), (1, 8))),
        "mix_lambda": jnp.clip(0.3 + 0.5 * jax.random.uniform(key_of[5], (HEADS,), jnp.float32) ** block_levels(key_of[5], (HEADS,), ((0, 8),), -0.2, 0.2), 0.3, 0.8),
        "head_gain": jnp.clip(1.0 + 0.18 * jax.random.normal(key_of[6], (2 * DH,), jnp.float32), 0.1, 1.9),
        "w_output": gaussian(key_of[7], (HEADS * 2 * DH, D), (HEADS * 2 * DH) ** -0.5, 0.125, ((0, 8),)),
        "cache_keys": draw_cache_keys(jax.random.fold_in(key_of[19], 71), 0),
        "cache_value": gaussian(key_of[9], (BATCH, CACHE, HEADS * 2 * DH), 1.0, 6.0, ((0, 4), (2, 8))),
        "lengths": touch_ends(jax.random.randint(key_of[10], (BATCH,), 1, CACHE + 1), jax.random.fold_in(key_of[10], 1), 1, CACHE).astype(jnp.int32),
        "moe_gain": jnp.clip(1.0 + 0.18 * jax.random.normal(key_of[11], (D,), jnp.float32), 0.1, 1.9),
        "group_ids": draw_group_ids(jax.random.fold_in(key_of[19], 71), 0),
        "member_ids": draw_member_ids(jax.random.fold_in(key_of[19], 71), 0),
        "group_gate": jnp.clip(0.3 + 0.7 * jax.random.uniform(key_of[14], (BATCH,), jnp.float32) ** block_levels(key_of[14], (BATCH,), ((0, 4),), -0.2, 0.2), 0.3, 1.0),
        "member_logits": gaussian(key_of[15], (BATCH, TOPK), 1.0, 4.0, ((0, 4),), jnp.float32),
        "w_exp_gate": gaussian(key_of[16], (EXPERTS, D, FF), D ** -0.5, 0.09375, ((0, 4), (2, 8))),
        "w_exp_up": gaussian(key_of[17], (EXPERTS, D, FF), D ** -0.5, 0.09375, ((0, 4), (2, 8))),
        "w_exp_down": gaussian(key_of[18], (EXPERTS, FF, D), FF ** -0.5, 0.125, ((0, 4), (1, 8))),
    }


EPS = 1e-06

def rms_scale(values, gain):
    return values * lax.rsqrt(lax.optimization_barrier(jnp.mean(values * values, axis=-1, keepdims=True)) + EPS) * gain

def reference(tokens, attn_gain, w_query, w_key, w_value, mix_lambda, head_gain, w_output, cache_keys, cache_value, lengths, moe_gain, group_ids, member_ids, group_gate, member_logits, w_exp_gate, w_exp_up, w_exp_down):
    resid_in = tokens.astype(jnp.float32)
    normed = rms_scale(resid_in, attn_gain).astype(jnp.bfloat16)

    def project(weight):
        return jnp.dot(normed, weight, preferred_element_type=jnp.float32).astype(jnp.bfloat16)
    query = project(w_query)
    fresh_keys = project(w_key)
    fresh_val = project(w_value)
    head_index = jnp.arange(HEADS).astype(jnp.float32)
    slopes = 2.0 ** (-8.0 * (head_index + 1.0) / HEADS)
    scale = DH ** (-0.5)
    lam = mix_lambda.astype(jnp.float32)

    def block(args):
        qry, knew, vnew, ckeys, cval, lens = args
        count = qry.shape[0]
        positions = jnp.arange(CACHE)
        dist = (lens[:, None] - positions[None, :]).astype(jnp.float32)
        valid = positions[None, :] < lens[:, None]
        qf = qry.reshape(count, HEADS, 2, DH).astype(jnp.float32)
        keys = ckeys.reshape(count, CACHE, HEADS, 2, DH).astype(jnp.float32)
        fresh = knew.reshape(count, HEADS, 2, DH).astype(jnp.float32)
        old = jnp.einsum('shcd,slhcd->cshl', qf, keys, precision=lax.Precision.HIGHEST) * scale
        old = old - slopes[None, None, :, None] * dist[None, :, None, :]
        old = jnp.where(valid[None, :, None, :], old, -jnp.inf)
        new = jnp.moveaxis(lax.optimization_barrier(jnp.sum(qf * fresh, axis=-1)) * scale, 2, 0)
        full = jnp.concatenate([old, new[..., None]], axis=-1)
        maps = jax.nn.softmax(full, axis=-1)
        weights = (maps[0] - lam[None, :, None] * maps[1]).astype(jnp.bfloat16)
        values = cval.reshape(count, CACHE, HEADS, 2 * DH).astype(jnp.float32)
        wide = weights.astype(jnp.float32)
        head_mix = jnp.einsum('shl,slhe->she', wide[..., :CACHE], values, precision=lax.Precision.HIGHEST)
        head_mix = head_mix + wide[..., CACHE][..., None] * vnew.reshape(count, HEADS, 2 * DH).astype(jnp.float32)
        head_out = rms_scale(head_mix, head_gain).astype(jnp.bfloat16)
        return head_out.reshape(count, HEADS * 2 * DH)

    def split(array):
        return array.reshape((N_EP, SEQ_DEV) + array.shape[1:])
    pieces = (split(query), split(fresh_keys), split(fresh_val), split(cache_keys), split(cache_value), split(lengths))
    head_out = lax.map(block, pieces).reshape(BATCH, HEADS * 2 * DH)
    group = HEADS * 2 * DH // N_TP
    attn_sum = jnp.zeros((BATCH, D), jnp.float32)
    for index in range(N_TP):
        term = jnp.dot(head_out[:, index * group:(index + 1) * group], w_output[index * group:(index + 1) * group], preferred_element_type=jnp.float32).astype(jnp.bfloat16)
        attn_sum = attn_sum + lax.optimization_barrier(term).astype(jnp.float32)
    resid = resid_in + attn_sum
    moe_in = rms_scale(resid, moe_gain).astype(jnp.bfloat16)
    expert_ids = group_ids[:, None] * EPG + member_ids
    route_weight = jax.nn.softmax(member_logits.astype(jnp.float32), axis=-1) * group_gate[:, None]

    def step(total, args):
        gate_w, up_w, down_w, index = args
        gate = jnp.dot(moe_in, gate_w, preferred_element_type=jnp.float32)
        upper = jnp.dot(moe_in, up_w, preferred_element_type=jnp.float32)
        hidden = (jax.nn.silu(gate) * upper).astype(jnp.bfloat16)
        result = jnp.dot(hidden, down_w, preferred_element_type=jnp.float32).astype(jnp.bfloat16)
        share = lax.optimization_barrier(jnp.sum(jnp.where(expert_ids == index, route_weight, 0.0), axis=1))
        return (total + share[:, None] * lax.optimization_barrier(result).astype(jnp.float32), None)
    routed, _ = lax.scan(step, jnp.zeros((BATCH, D), jnp.float32), (w_exp_gate, w_exp_up, w_exp_down, jnp.arange(EXPERTS).astype(jnp.int32)))
    mixed = (resid + routed).astype(jnp.bfloat16)
    return (mixed, fresh_keys, fresh_val)
```

```python
import functools

import jax
import jax.numpy as jnp
from jax import lax
from jax.experimental import pallas as pl
from jax.experimental.pallas import tpu as pltpu
from jax.sharding import PartitionSpec as P

EPG = 2
EPS = 1e-06
MESH = pl.DeviceIdType.MESH
F32 = jnp.float32
BF16 = jnp.bfloat16
LOAD = 4
ROWS = 8


def iota(shape, dim):
    return lax.broadcasted_iota(jnp.int32, shape, dim)


def roll_rows(x, shift):
    shift = shift % ROWS
    return pltpu.roll(x, shift, 0) if shift else x


def mm(a, b):
    return jnp.dot(a, b, preferred_element_type=F32)


def layer_kernel(
    n_ep, n_tp,
    tokens_h, attn_gain_h, head_gain_h, moe_gain_h, lam_h, lengths_h, groups_h, groups_row_h, members_h, gate_h, logits_h,
    w_query, w_key, w_value, cache_keys, cache_value, w_output, w_gate, w_up, w_down,
    mixed, fresh_keys, fresh_value,
    tokens, attn_gain, head_gain, moe_gain, lam, lengths, groups, groups_row, members, group_gate, logits,
    wq, wk, wv, kbuf, vbuf, ktrans, wo, wg, wu, wd,
    nsend, nrecv, qpart, kvpart, qprecv, kvprecv, mixbuf,
    tsend, trecv, dsend, drecv, ssend, srecv, csend, crecv,
    i_sem, w_sem, c_sem, n_ss, n_rs, p_ss, p_rs, t_ss, t_rs, d_ss, d_rs, d0_rs, s_ss, s_rs, s0_rs, e_ss, e_rs, e0_rs,
):
    ep = lax.axis_index("ep")
    tp = lax.axis_index("tp")
    seqs, width = tokens.shape
    rows_local = width // n_ep
    qk_cols = w_query.shape[1]
    heads_local = lam.shape[0]
    pair = qk_cols // heads_local
    head_dim = pair // 2
    total_heads = heads_local * n_tp
    positions = cache_keys.shape[1]
    cols = width // n_tp
    waves = seqs // ROWS
    n_groups = n_ep // EPG
    hc = ROWS // n_groups
    colsp = dsend.shape[-1]
    pack = cols // colsp
    batch = ROWS // heads_local
    slots = n_ep * ROWS

    oe = [lax.rem(ep + d, n_ep) for d in range(n_ep)]
    ot = [lax.rem(tp + d, n_tp) for d in range(n_tp)]

    barrier = pltpu.get_barrier_semaphore()
    for d in range(1, n_tp):
        pl.semaphore_signal(barrier, inc=1, device_id={"ep": ep, "tp": ot[d]}, device_id_type=MESH)
    for d in range(1, n_ep):
        pl.semaphore_signal(barrier, inc=1, device_id={"ep": oe[d], "tp": tp}, device_id_type=MESH)

    small = [
        (tokens_h, tokens), (attn_gain_h, attn_gain), (head_gain_h, head_gain), (moe_gain_h, moe_gain), (lam_h, lam),
        (lengths_h, lengths), (groups_h, groups), (groups_row_h, groups_row), (members_h, members),
        (gate_h, group_gate), (logits_h, logits),
    ]
    small_copies = [pltpu.make_async_copy(s, d, i_sem.at[i]) for i, (s, d) in enumerate(small)]
    for c in small_copies:
        c.start()
    weight_pairs = [(w_query, wq), (w_key, wk), (w_value, wv), (w_output, wo), (w_gate, wg), (w_up, wu), (w_down, wd)]
    weight_copies = [pltpu.make_async_copy(s, d, w_sem.at[i]) for i, (s, d) in enumerate(weight_pairs)]

    def cache_copy(g, kind):
        src, dst = ((cache_keys, kbuf), (cache_value, vbuf))[kind]
        rows = pl.ds(g * LOAD, LOAD)
        return pltpu.make_async_copy(src.at[rows], dst.at[rows], c_sem.at[kind, g])

    for i in range(3):
        weight_copies[i].start(priority=1)
    for kind in range(2):
        for g in range(seqs // LOAD):
            cache_copy(g, kind).start(priority=1)
    for i in range(3, 7):
        weight_copies[i].start(priority=1)

    small_copies[0].wait()
    small_copies[1].wait()
    resid_in = tokens[...].astype(F32)
    inv = lax.rsqrt(jnp.mean(resid_in * resid_in, axis=-1, keepdims=True) + EPS)
    normed = (resid_in * inv * attn_gain[...]).astype(BF16)
    for e in range(n_ep):
        nsend[e] = normed[:, e * rows_local : (e + 1) * rows_local]

    def remote(src, dst, ss, rs, e, t):
        return pltpu.make_async_remote_copy(
            src_ref=src, dst_ref=dst, send_sem=ss, recv_sem=rs, device_id={"ep": e, "tp": t}, device_id_type=MESH
        )

    pl.semaphore_wait(barrier, n_ep + n_tp - 2)
    n_copies = [
        remote(nsend.at[oe[d]], nrecv.at[d], n_ss.at[d], n_rs.at[d], oe[d], tp) for d in range(1, n_ep)
    ]
    for c in n_copies:
        c.start()
    nrecv[0] = nsend[ep]

    eye = (iota((qk_cols, qk_cols), 0) == iota((qk_cols, qk_cols), 1)).astype(BF16)

    def turn(s, carry):
        flipped = lax.dot_general(eye, kbuf[s], (((1,), (1,)), ((), ())), preferred_element_type=F32)
        ktrans[s] = flipped.astype(BF16)
        return carry

    def turn_group(g, carry):
        cache_copy(g, 0).wait()
        lax.fori_loop(g * LOAD, (g + 1) * LOAD, turn, 0)
        return carry

    half = seqs // LOAD // 2
    lax.fori_loop(0, half, turn_group, 0)

    for c in weight_copies[:3]:
        c.wait()
    for c in n_copies:
        c.wait_recv()
    rows_all = nrecv[...].reshape(n_ep * seqs, rows_local)
    p_copies = []
    for i, w in enumerate((wq, wk, wv)):
        part = mm(rows_all, w[...]).reshape(n_ep, seqs, qk_cols)
        if i == 0:
            qpart[...] = part
        else:
            kvpart[:, :, (i - 1) * qk_cols : i * qk_cols] = part.astype(BF16)
    back = [lax.rem(ep + n_ep - d, n_ep) for d in range(n_ep)]
    for d in range(1, n_ep):
        p_copies.append(remote(qpart.at[d], qprecv.at[d], p_ss.at[0, d], p_rs.at[0, d], back[d], tp))
        p_copies.append(remote(kvpart.at[d], kvprecv.at[d], p_ss.at[1, d], p_rs.at[1, d], back[d], tp))
    for c in p_copies:
        c.start()

    lax.fori_loop(half, seqs // LOAD, turn_group, 0)

    for c in small_copies[2:]:
        c.wait()
    same_index = iota((seqs, seqs), 0) == iota((seqs, seqs), 1)

    def column(row):
        return jnp.sum(jnp.where(same_index, row, 0.0), axis=1, keepdims=True)

    group_row = groups_row[...].astype(F32)
    group_col = column(group_row)
    earlier = (group_col == group_row) & (iota((seqs, seqs), 0) < iota((seqs, seqs), 1))
    rank_row = jnp.sum(earlier.astype(F32), axis=0, keepdims=True)
    wave_row = jnp.floor(rank_row / hc)
    place_row = wave_row * ROWS + group_row * hc + (rank_row - wave_row * hc)
    place_col = column(place_row)
    to_place = (place_row == iota((seqs, seqs), 0).astype(F32)).astype(BF16)
    from_place = (place_col == iota((seqs, seqs), 1).astype(F32)).astype(BF16)

    ranks = []
    group_of = [groups[s] for s in range(seqs)]
    for s in range(seqs):
        r = jnp.int32(0)
        for before in range(s):
            r = r + jnp.where(group_of[before] == group_of[s], 1, 0)
        ranks.append(r)
    places = [(ranks[s] // hc) * ROWS + group_of[s] * hc + ranks[s] % hc for s in range(seqs)]
    perm = []
    for p in range(seqs):
        at = jnp.int32(0)
        for s in range(seqs):
            at = at + jnp.where(places[s] == p, s, 0)
        perm.append(at)

    lg = logits[...]
    ex = jnp.exp(lg - jnp.max(lg, axis=0, keepdims=True))
    route_rows = ex / jnp.sum(ex, axis=0, keepdims=True) * group_gate[...]
    shares = []
    for m in range(EPG):
        hit = (members[...] == m).astype(F32)
        shares.append(jnp.sum(route_rows * hit, axis=0, keepdims=True))
    row_col = iota((ROWS, 1), 0)
    slot_col = row_col % hc if pack == 2 else row_col

    def share_col(w, g, m):
        wanted = (w * ROWS + g * hc + slot_col).astype(F32)
        return jnp.sum(jnp.where(place_row == wanted, shares[m], 0.0), axis=1, keepdims=True)

    weights_of = [
        [[share_col(w, g, m) for m in range(EPG)] for g in range(n_groups)] for w in range(waves)
    ]

    my_cols = pl.ds(pl.multiple_of(tp * cols, cols), cols)
    placed_tokens = mm(to_place, tokens[:, my_cols])
    gain_part = moe_gain[:, my_cols]

    scale = head_dim ** (-0.5)
    row16 = iota((2 * ROWS, qk_cols), 0)
    col16 = iota((2 * ROWS, qk_cols), 1)
    head16 = row16 % heads_local
    map_mask = ((col16 // pair == head16) & ((col16 // head_dim) % 2 == row16 // ROWS)).astype(F32)
    seq16 = (row16 % ROWS) // heads_local
    head8 = iota((ROWS, qk_cols), 0) % heads_local
    head_mask = (iota((ROWS, qk_cols), 1) // pair == head8).astype(F32)
    seq8 = iota((ROWS, qk_cols), 0) // heads_local
    row_id = iota((2 * ROWS, 1), 0)
    slopes = jnp.exp2(-8.0 * ((tp * heads_local + row_id % heads_local).astype(F32) + 1.0) / total_heads)
    lam_col = jnp.zeros((ROWS, 1), F32)
    for h in range(heads_local):
        lam_col = jnp.where(row_col % heads_local == h, lam[h], lam_col)
    gain_row = jnp.concatenate([head_gain[...]] * heads_local, axis=1)
    spots = iota((1, positions), 1)
    pick16 = (row_id % ROWS) // heads_local

    for g in range(seqs // LOAD):
        cache_copy(g, 1).wait()

    for c in p_copies:
        c.wait_recv()
    query = qpart[0]
    fresh = kvpart[0].astype(F32)
    for d in range(1, n_ep):
        query = query + qprecv[d]
        fresh = fresh + kvprecv[d].astype(F32)
    fresh = fresh.astype(BF16)
    fresh_keys[...] = fresh[:, :qk_cols]
    fresh_value[...] = fresh[:, qk_cols:]
    projected = jnp.concatenate([query.astype(BF16), fresh], axis=1)

    weight_copies[3].wait()

    def attend(base):
        wanted = (base + pick16).astype(F32)
        spread = mm((place_row == wanted).astype(BF16), projected)
        q16 = spread[:, :qk_cols] * map_mask
        lens = jnp.zeros((2 * ROWS, 1), jnp.int32)
        old = None
        for i in range(batch):
            at = perm[base + i]
            lens = jnp.where(pick16 == i, lengths[at], lens)
            own = jnp.where(seq16 == i, q16, 0.0).astype(BF16)
            part = mm(own, ktrans[at])
            old = part if old is None else old + part
        new = jnp.sum(q16 * spread[:, qk_cols : 2 * qk_cols], axis=-1, keepdims=True) * scale
        old = old * scale - slopes * (lens - spots).astype(F32)
        old = jnp.where(spots < lens, old, -jnp.inf)
        top = jnp.maximum(jnp.max(old, axis=-1, keepdims=True), new)
        old = jnp.exp(old - top)
        new = jnp.exp(new - top)
        recip = 1.0 / (jnp.sum(old, axis=-1, keepdims=True) + new)
        old = old * recip
        new = new * recip
        weights = (old[:ROWS] - lam_col * old[ROWS:]).astype(BF16)
        fresh_weight = (new[:ROWS] - lam_col * new[ROWS:]).astype(BF16).astype(F32)
        mix = fresh_weight * spread[:ROWS, 2 * qk_cols :]
        for i in range(batch):
            part = mm(weights, vbuf[perm[base + i]])
            mix = mix + jnp.where(seq8 == i, part, 0.0)
        mix = mix * head_mask
        mean = jnp.sum(mix * mix, axis=-1, keepdims=True) / pair
        return mix * lax.rsqrt(mean + EPS) * gain_row

    t_copies = [[] for _ in range(waves)]
    for w in range(waves):
        per_wave = ROWS // batch
        for k in range(per_wave):
            mix = attend(w * ROWS + k * batch)
            for h in range(heads_local):
                mixbuf[w * heads_local + h, k * ROWS : (k + 1) * ROWS, :] = mix[:, h * pair : (h + 1) * pair]
        heads = [
            mixbuf[w * heads_local + h, pl.ds(h, ROWS, stride=heads_local), :] for h in range(heads_local)
        ]
        heads = jnp.concatenate(heads, axis=1).astype(BF16)
        for d in [*range(1, n_tp), 0]:
            block = wo[:, pl.ds(pl.multiple_of(ot[d] * cols, cols), cols)]
            term = mm(heads, block).astype(BF16)
            if d:
                tsend[w, d] = term
                c = remote(tsend.at[w, d], trecv.at[w, d], t_ss.at[w, d], t_rs.at[w, d], ep, ot[d])
                c.start()
                t_copies[w].append(c)
            else:
                trecv[w, 0] = term

    rows_of = iota((ROWS, colsp), 0)
    resid = []
    d_copies = [[] for _ in range(waves)]
    for w in range(waves):
        for c in t_copies[w]:
            c.wait_recv()
        attn = trecv[w, 0].astype(F32)
        for d in range(1, n_tp):
            attn = attn + trecv[w, d].astype(F32)
        res = placed_tokens[w * ROWS : (w + 1) * ROWS] + attn
        resid.append(res)
        rows = res * gain_part
        for g in range(n_groups):
            if pack == 2:
                first = roll_rows(rows[:, :colsp], -g * hc)
                second = roll_rows(rows[:, colsp:], hc - g * hc)
                dsend[w, g] = jnp.where(rows_of < hc, first, second).astype(BF16)
            else:
                dsend[w, g] = roll_rows(rows, -g * hc).astype(BF16)
        squares = jnp.sum(res * res, axis=-1, keepdims=True)
        wide = jnp.where(iota((ROWS, 128), 0) == iota((ROWS, 128), 1), squares, 0.0)
        ssend[w] = jnp.sum(wide, axis=0, keepdims=True)
        for t in [*range(1, n_tp), 0]:
            for e in range(n_ep):
                if t or e:
                    d_rs_at = d_rs.at[w, t] if t else d0_rs.at[w, e]
                    s_rs_at = s_rs.at[w, t] if t else s0_rs.at[w, e]
                    c = remote(dsend.at[w, oe[e] // EPG], drecv.at[w, t, e], d_ss.at[w, t, e], d_rs_at, oe[e], ot[t])
                    c.start()
                    s = remote(ssend.at[w], srecv.at[w, t, e], s_ss.at[w, t, e], s_rs_at, oe[e], ot[t])
                    s.start()
                    d_copies[w] += [c, s]
        drecv[w, 0, 0] = dsend[w, ep // EPG]
        srecv[w, 0, 0] = ssend[w]

    def slab_wait(ref, sem):
        pltpu.make_async_copy(ref, ref, sem).wait()

    e_copies = [[] for _ in range(waves)]
    rows32 = iota((slots, w_gate.shape[2]), 0) % ROWS
    for i in range(4, 7):
        weight_copies[i].wait()
    for w in range(waves):
        hid = w_gate.shape[2]
        gates = [jnp.zeros((slots, hid), F32) for _ in range(pack)]
        uppers = [jnp.zeros((slots, hid), F32) for _ in range(pack)]
        for t in range(n_tp):
            if t:
                slab_wait(drecv.at[w, t], d_rs.at[w, t])
            else:
                for e in range(1, n_ep):
                    slab_wait(drecv.at[w, 0, e], d0_rs.at[w, e])
            x = drecv[w, t].reshape(slots, colsp)
            source = lax.rem(tp + n_tp - t, n_tp)
            for p in range(pack):
                at = pl.ds(pl.multiple_of(source * cols + p * colsp, colsp), colsp)
                gates[p] = gates[p] + mm(x, wg[0, at])
                uppers[p] = uppers[p] + mm(x, wu[0, at])
        for t in range(n_tp):
            if t:
                slab_wait(srecv.at[w, t], s_rs.at[w, t])
            else:
                for e in range(1, n_ep):
                    slab_wait(srecv.at[w, 0, e], s0_rs.at[w, e])
        squares = srecv[w, 0]
        for t in range(1, n_tp):
            squares = squares + srecv[w, t]
        squares = jnp.broadcast_to(squares, (n_ep, ROWS, 128)).reshape(slots, 128)
        slot = iota((slots, 128), 0) % ROWS
        if pack == 2:
            slot = slot % hc
        lane = (ep // EPG) * hc + slot
        lane = lax.rem(lane, ROWS)
        squares = jnp.sum(jnp.where(iota((slots, 128), 1) == lane, squares, 0.0), axis=-1, keepdims=True)
        inv = lax.rsqrt(squares / width + EPS)

        def join(parts):
            if pack == 1:
                return parts[0]
            down_shift = pltpu.roll(parts[1], slots - hc, 0)
            up_shift = pltpu.roll(parts[0], hc, 0)
            return jnp.where(rows32 < hc, parts[0] + down_shift, parts[1] + up_shift)

        gate = join(gates) * inv
        upper = join(uppers) * inv
        hidden = (gate / (1.0 + jnp.exp(-gate)) * upper).astype(BF16)
        for t in [*range(1, n_tp), 0]:
            downs = [
                mm(hidden, wd[0, :, pl.ds(pl.multiple_of(ot[t] * cols + p * colsp, colsp), colsp)]) for p in range(pack)
            ]
            down = downs[0] if pack == 1 else jnp.where(iota((slots, colsp), 0) % ROWS < hc, downs[0], downs[1])
            down = down.reshape(n_ep, ROWS, colsp).astype(BF16)
            csend[w, t] = down
            for e in range(n_ep):
                if t or e:
                    e_rs_at = e_rs.at[w, t] if t else e0_rs.at[w, e]
                    c = remote(csend.at[w, t, e], crecv.at[w, t, ep], e_ss.at[w, t, e], e_rs_at, back[e], ot[t])
                    c.start()
                    e_copies[w].append(c)
        crecv[w, 0, ep] = csend[w, 0, 0]

    for c in n_copies + p_copies:
        c.wait_send()
    for w in range(waves):
        for c in t_copies[w] + d_copies[w] + e_copies[w]:
            c.wait_send()

    final = None
    for w in range(waves):
        for t in range(n_tp):
            if t:
                slab_wait(crecv.at[w, t], e_rs.at[w, t])
            else:
                for e in range(1, n_ep):
                    slab_wait(crecv.at[w, 0, e], e0_rs.at[w, e])
        routed = [jnp.zeros((ROWS, colsp), F32) for _ in range(pack)]
        for g in range(n_groups):
            total = jnp.zeros((ROWS, colsp), F32)
            for m in range(EPG):
                e = g * EPG + m
                out = crecv[w, 0, e].astype(F32)
                for t in range(1, n_tp):
                    out = out + crecv[w, t, e].astype(F32)
                total = total + weights_of[w][g][m] * out.astype(BF16).astype(F32)
            for p in range(pack):
                routed[p] = jnp.where(rows_of // hc == g, roll_rows(total, g * hc - p * hc), routed[p])
        routed = routed[0] if pack == 1 else jnp.concatenate(routed, axis=1)
        placed = (resid[w] + routed).astype(BF16)
        part = mm(from_place[:, w * ROWS : (w + 1) * ROWS], placed)
        final = part if final is None else final + part
    mixed[...] = final.astype(BF16)


def finish_kernel(a, b, c, x, y, z):
    x[...] = a[...]
    y[...] = b[...]
    z[...] = c[...]


def on_device(
    tokens, attn_gain, w_query, w_key, w_value, mix_lambda, head_gain, w_output, cache_keys, cache_value,
    lengths, moe_gain, group_ids, member_ids, group_gate, member_logits, w_exp_gate, w_exp_up, w_exp_down,
):
    n_ep, n_tp = lax.axis_size("ep"), lax.axis_size("tp")
    seqs, width = tokens.shape
    qk_cols = w_query.shape[1]
    heads_local = mix_lambda.shape[0]
    cols = width // n_tp
    waves = seqs // ROWS
    n_groups = n_ep // EPG
    hc = ROWS // n_groups
    pack = 2 if hc * 2 == ROWS and cols % 256 == 0 else 1
    colsp = cols // pack
    vmem = pl.BlockSpec(memory_space=pltpu.VMEM)
    hbm = pl.BlockSpec(memory_space=pl.ANY)
    dma = pltpu.SemaphoreType.DMA
    like = lambda a: pltpu.VMEM(a.shape, a.dtype)
    operands = (
        tokens, attn_gain[None, :], head_gain[None, :], moe_gain[None, :], mix_lambda, lengths, group_ids,
        group_ids[None, :], member_ids.T, group_gate[None, :], member_logits.T,
        w_query, w_key, w_value, cache_keys, cache_value, w_output, w_exp_gate, w_exp_up, w_exp_down,
    )
    held = [
        pltpu.SMEM(a.shape, a.dtype) if i in (4, 5, 6) else like(a) for i, a in enumerate(operands[:11])
    ]
    scratch = held + [
        like(w_query), like(w_key), like(w_value), like(cache_keys), like(cache_value),
        pltpu.VMEM((seqs, qk_cols, cache_keys.shape[1]), BF16),
        like(w_output), like(w_exp_gate), like(w_exp_up), like(w_exp_down),
        pltpu.VMEM((n_ep, seqs, width // n_ep), BF16),
        pltpu.VMEM((n_ep, seqs, width // n_ep), BF16),
        pltpu.VMEM((n_ep, seqs, qk_cols), F32),
        pltpu.VMEM((n_ep, seqs, 2 * qk_cols), BF16),
        pltpu.VMEM((n_ep, seqs, qk_cols), F32),
        pltpu.VMEM((n_ep, seqs, 2 * qk_cols), BF16),
        pltpu.VMEM((waves * heads_local, ROWS * heads_local, qk_cols // heads_local), F32),
        pltpu.VMEM((waves, n_tp, ROWS, cols), BF16),
        pltpu.VMEM((waves, n_tp, ROWS, cols), BF16),
        pltpu.VMEM((waves, n_groups, ROWS, colsp), BF16),
        pltpu.VMEM((waves, n_tp, n_ep, ROWS, colsp), BF16),
        pltpu.VMEM((waves, 1, 128), F32),
        pltpu.VMEM((waves, n_tp, n_ep, 1, 128), F32),
        pltpu.VMEM((waves, n_tp, n_ep, ROWS, colsp), BF16),
        pltpu.VMEM((waves, n_tp, n_ep, ROWS, colsp), BF16),
        dma((11,)), dma((7,)), dma((2, seqs // LOAD)),
        dma((n_ep,)), dma((n_ep,)), dma((2, n_ep)), dma((2, n_ep)),
        dma((waves, n_tp)), dma((waves, n_tp)),
        dma((waves, n_tp, n_ep)), dma((waves, n_tp)), dma((waves, n_ep)),
        dma((waves, n_tp, n_ep)), dma((waves, n_tp)), dma((waves, n_ep)),
        dma((waves, n_tp, n_ep)), dma((waves, n_tp)), dma((waves, n_ep)),
    ]
    shapes = (
        jax.ShapeDtypeStruct((seqs, cols), BF16),
        jax.ShapeDtypeStruct((seqs, qk_cols), BF16),
        jax.ShapeDtypeStruct((seqs, qk_cols), BF16),
    )
    results = pl.pallas_call(
        functools.partial(layer_kernel, n_ep, n_tp),
        out_shape=shapes,
        in_specs=[hbm] * len(operands),
        out_specs=(vmem, vmem, vmem),
        scratch_shapes=scratch,
        compiler_params=pltpu.CompilerParams(
            collective_id=0, has_side_effects=True, vmem_limit_bytes=60 * 1024 * 1024
        ),
        name="decode_layer",
    )(*operands)
    return pl.pallas_call(
        finish_kernel, out_shape=shapes, in_specs=[vmem] * 3, out_specs=(vmem,) * 3, name="finish"
    )(*results)


def solution(mesh):
    return jax.shard_map(
        on_device,
        mesh=mesh,
        in_specs=(
            P("ep", None),
            P(),
            P("ep", "tp"),
            P("ep", "tp"),
            P("ep", "tp"),
            P("tp"),
            P(),
            P("tp", None),
            P("ep", None, "tp"),
            P("ep", None, "tp"),
            P("ep"),
            P(),
            P("ep"),
            P("ep", None),
            P("ep"),
            P("ep", None),
            P("ep", None, "tp"),
            P("ep", None, "tp"),
            P("ep", "tp", None),
        ),
        out_specs=(P("ep", "tp"), P("ep", "tp"), P("ep", "tp")),
        check_vma=False,
    )
```

```python
import functools

import jax
import jax.numpy as jnp
from jax import lax
from jax.experimental import pallas as pl
from jax.experimental.pallas import tpu as pltpu
from jax.sharding import PartitionSpec as P

EPG = 2
EPS = 1e-06
MESH = pl.DeviceIdType.MESH
F32 = jnp.float32
BF16 = jnp.bfloat16
LOAD = 4
ROWS = 8


def iota(shape, dim):
    return lax.broadcasted_iota(jnp.int32, shape, dim)


def roll_rows(x, shift):
    shift = shift % ROWS
    return pltpu.roll(x, shift, 0) if shift else x


def mm(a, b):
    return jnp.dot(a, b, preferred_element_type=F32)


def layer_kernel(
    n_ep, n_tp,
    tokens_h, attn_gain_h, head_gain_h, moe_gain_h, lam_h, lengths_h, groups_h, groups_row_h, members_h, gate_h, logits_h,
    w_query, w_key, w_value, cache_keys, cache_value, w_output, w_gate, w_up, w_down,
    mixed, fresh_keys, fresh_value,
    tokens, attn_gain, head_gain, moe_gain, lam, lengths, groups, groups_row, members, group_gate, logits,
    wq, wk, wv, kbuf, vbuf, ktrans, wo, wg, wu, wd,
    nsend, nrecv, qpart, kvpart, qprecv, kvprecv, mixbuf,
    tsend, trecv, dsend, drecv, ssend, srecv, csend, crecv,
    i_sem, w_sem, c_sem, n_sem, p_sem, t_sem, d_ss, d_rs, s_sem, e_sem,
):
    ep = lax.axis_index("ep")
    tp = lax.axis_index("tp")
    seqs, width = tokens.shape
    rows_local = width // n_ep
    qk_cols = w_query.shape[1]
    heads_local = lam.shape[0]
    pair = qk_cols // heads_local
    head_dim = pair // 2
    total_heads = heads_local * n_tp
    positions = cache_keys.shape[1]
    cols = width // n_tp
    waves = seqs // ROWS
    n_groups = n_ep // EPG
    hc = ROWS // n_groups
    colsp = dsend.shape[-1]
    pack = cols // colsp
    batch = ROWS // heads_local
    slots = n_ep * ROWS

    oe = [lax.rem(ep + d, n_ep) for d in range(n_ep)]
    ot = [lax.rem(tp + d, n_tp) for d in range(n_tp)]

    barrier = pltpu.get_barrier_semaphore()
    for d in range(1, n_tp):
        pl.semaphore_signal(barrier, inc=1, device_id={"ep": ep, "tp": ot[d]}, device_id_type=MESH)
    for d in range(1, n_ep):
        pl.semaphore_signal(barrier, inc=1, device_id={"ep": oe[d], "tp": tp}, device_id_type=MESH)

    small = [
        (tokens_h, tokens), (attn_gain_h, attn_gain), (head_gain_h, head_gain), (moe_gain_h, moe_gain), (lam_h, lam),
        (lengths_h, lengths), (groups_h, groups), (groups_row_h, groups_row), (members_h, members),
        (gate_h, group_gate), (logits_h, logits),
    ]
    small_copies = [pltpu.make_async_copy(s, d, i_sem.at[i]) for i, (s, d) in enumerate(small)]
    for c in small_copies:
        c.start()
    weight_pairs = [(w_query, wq), (w_key, wk), (w_value, wv), (w_output, wo), (w_gate, wg), (w_up, wu), (w_down, wd)]
    weight_copies = [pltpu.make_async_copy(s, d, w_sem.at[i]) for i, (s, d) in enumerate(weight_pairs)]

    def key_copy(g):
        rows = pl.ds(g * LOAD, LOAD)
        return pltpu.make_async_copy(cache_keys.at[rows], kbuf.at[rows], c_sem.at[g])

    value_copy = pltpu.make_async_copy(cache_value, vbuf, c_sem.at[seqs // LOAD])

    for i in range(3):
        weight_copies[i].start(priority=1)
    for g in range(seqs // LOAD):
        key_copy(g).start(priority=1)
    value_copy.start(priority=1)
    for i in range(3, 7):
        weight_copies[i].start(priority=1)

    small_copies[0].wait()
    small_copies[1].wait()
    resid_in = tokens[...].astype(F32)
    inv = lax.rsqrt(jnp.mean(resid_in * resid_in, axis=-1, keepdims=True) + EPS)
    normed = (resid_in * inv * attn_gain[...]).astype(BF16)
    for e in range(n_ep):
        nsend[e] = normed[:, e * rows_local : (e + 1) * rows_local]

    def remote(src, dst, ss, rs, e, t):
        return pltpu.make_async_remote_copy(
            src_ref=src, dst_ref=dst, send_sem=ss, recv_sem=rs, device_id={"ep": e, "tp": t}, device_id_type=MESH
        )

    pl.semaphore_wait(barrier, n_ep + n_tp - 2)
    def slab_wait(ref, sem):
        pltpu.make_async_copy(ref, ref, sem).wait()

    for d in range(1, n_ep):
        remote(nsend.at[oe[d]], nrecv.at[d], n_sem.at[0], n_sem.at[1], oe[d], tp).start()
    nrecv[0] = nsend[ep]

    eye = (iota((qk_cols, qk_cols), 0) == iota((qk_cols, qk_cols), 1)).astype(BF16)

    def turn(s, carry):
        flipped = lax.dot_general(eye, kbuf[s], (((1,), (1,)), ((), ())), preferred_element_type=F32)
        ktrans[s] = flipped.astype(BF16)
        return carry

    def turn_group(g, carry):
        key_copy(g).wait()
        lax.fori_loop(g * LOAD, (g + 1) * LOAD, turn, 0)
        return carry

    half = seqs // LOAD // 2
    lax.fori_loop(0, half, turn_group, 0)

    for c in weight_copies[:3]:
        c.wait()
    slab_wait(nrecv.at[1:n_ep], n_sem.at[1])
    rows_all = nrecv[...].reshape(n_ep * seqs, rows_local)
    for i, w in enumerate((wq, wk, wv)):
        part = mm(rows_all, w[...]).reshape(n_ep, seqs, qk_cols)
        if i == 0:
            qpart[...] = part
        else:
            kvpart[:, :, (i - 1) * qk_cols : i * qk_cols] = part.astype(BF16)
    back = [lax.rem(ep + n_ep - d, n_ep) for d in range(n_ep)]
    for d in range(1, n_ep):
        remote(qpart.at[d], qprecv.at[d], p_sem.at[0], p_sem.at[1], back[d], tp).start()
        remote(kvpart.at[d], kvprecv.at[d], p_sem.at[2], p_sem.at[3], back[d], tp).start()

    lax.fori_loop(half, seqs // LOAD, turn_group, 0)

    for c in small_copies[2:]:
        c.wait()
    same_index = iota((seqs, seqs), 0) == iota((seqs, seqs), 1)

    def column(row):
        return jnp.sum(jnp.where(same_index, row, 0.0), axis=1, keepdims=True)

    group_row = groups_row[...].astype(F32)
    group_col = column(group_row)
    earlier = (group_col == group_row) & (iota((seqs, seqs), 0) < iota((seqs, seqs), 1))
    rank_row = jnp.sum(earlier.astype(F32), axis=0, keepdims=True)
    wave_row = jnp.floor(rank_row / hc)
    place_row = wave_row * ROWS + group_row * hc + (rank_row - wave_row * hc)
    place_col = column(place_row)
    to_place = (place_row == iota((seqs, seqs), 0).astype(F32)).astype(BF16)
    from_place = (place_col == iota((seqs, seqs), 1).astype(F32)).astype(BF16)

    ranks = []
    group_of = [groups[s] for s in range(seqs)]
    for s in range(seqs):
        r = jnp.int32(0)
        for before in range(s):
            r = r + jnp.where(group_of[before] == group_of[s], 1, 0)
        ranks.append(r)
    places = [(ranks[s] // hc) * ROWS + group_of[s] * hc + ranks[s] % hc for s in range(seqs)]
    perm = []
    for p in range(seqs):
        at = jnp.int32(0)
        for s in range(seqs):
            at = at + jnp.where(places[s] == p, s, 0)
        perm.append(at)

    lg = logits[...]
    ex = jnp.exp(lg - jnp.max(lg, axis=0, keepdims=True))
    route_rows = ex / jnp.sum(ex, axis=0, keepdims=True) * group_gate[...]
    shares = []
    for m in range(EPG):
        hit = (members[...] == m).astype(F32)
        shares.append(jnp.sum(route_rows * hit, axis=0, keepdims=True))
    row_col = iota((ROWS, 1), 0)
    slot_col = row_col % hc if pack == 2 else row_col

    def share_col(w, g, m):
        wanted = (w * ROWS + g * hc + slot_col).astype(F32)
        return jnp.sum(jnp.where(place_row == wanted, shares[m], 0.0), axis=1, keepdims=True)

    weights_of = [
        [[share_col(w, g, m) for m in range(EPG)] for g in range(n_groups)] for w in range(waves)
    ]

    my_cols = pl.ds(pl.multiple_of(tp * cols, cols), cols)
    placed_tokens = mm(to_place, tokens[:, my_cols])
    gain_part = moe_gain[:, my_cols]

    scale = head_dim ** (-0.5)
    row16 = iota((2 * ROWS, qk_cols), 0)
    col16 = iota((2 * ROWS, qk_cols), 1)
    head16 = row16 % heads_local
    map_mask = ((col16 // pair == head16) & ((col16 // head_dim) % 2 == row16 // ROWS)).astype(F32)
    seq16 = (row16 % ROWS) // heads_local
    head8 = iota((ROWS, qk_cols), 0) % heads_local
    head_mask = (iota((ROWS, qk_cols), 1) // pair == head8).astype(F32)
    seq8 = iota((ROWS, qk_cols), 0) // heads_local
    row_id = iota((2 * ROWS, 1), 0)
    slopes = jnp.exp2(-8.0 * ((tp * heads_local + row_id % heads_local).astype(F32) + 1.0) / total_heads)
    lam_col = jnp.zeros((ROWS, 1), F32)
    for h in range(heads_local):
        lam_col = jnp.where(row_col % heads_local == h, lam[h], lam_col)
    gain_row = jnp.concatenate([head_gain[...]] * heads_local, axis=1)
    spots = iota((1, positions), 1)
    pick16 = (row_id % ROWS) // heads_local

    value_copy.wait()

    slab_wait(qprecv.at[1:n_ep], p_sem.at[1])
    slab_wait(kvprecv.at[1:n_ep], p_sem.at[3])
    query = qpart[0]
    fresh = kvpart[0].astype(F32)
    for d in range(1, n_ep):
        query = query + qprecv[d]
        fresh = fresh + kvprecv[d].astype(F32)
    fresh = fresh.astype(BF16)
    fresh_keys[...] = fresh[:, :qk_cols]
    fresh_value[...] = fresh[:, qk_cols:]
    projected = jnp.concatenate([query.astype(BF16), fresh], axis=1)

    weight_copies[3].wait()

    def attend(base):
        wanted = (base + pick16).astype(F32)
        spread = mm((place_row == wanted).astype(BF16), projected)
        q16 = spread[:, :qk_cols] * map_mask
        lens = jnp.zeros((2 * ROWS, 1), jnp.int32)
        old = None
        for i in range(batch):
            at = perm[base + i]
            lens = jnp.where(pick16 == i, lengths[at], lens)
            own = jnp.where(seq16 == i, q16, 0.0).astype(BF16)
            part = mm(own, ktrans[at])
            old = part if old is None else old + part
        new = jnp.sum(q16 * spread[:, qk_cols : 2 * qk_cols], axis=-1, keepdims=True) * scale
        old = old * scale - slopes * (lens - spots).astype(F32)
        old = jnp.where(spots < lens, old, -jnp.inf)
        top = jnp.maximum(jnp.max(old, axis=-1, keepdims=True), new)
        old = jnp.exp(old - top)
        new = jnp.exp(new - top)
        recip = 1.0 / (jnp.sum(old, axis=-1, keepdims=True) + new)
        old = old * recip
        new = new * recip
        weights = (old[:ROWS] - lam_col * old[ROWS:]).astype(BF16)
        fresh_weight = (new[:ROWS] - lam_col * new[ROWS:]).astype(BF16).astype(F32)
        mix = fresh_weight * spread[:ROWS, 2 * qk_cols :]
        for i in range(batch):
            part = mm(weights, vbuf[perm[base + i]])
            mix = mix + jnp.where(seq8 == i, part, 0.0)
        mix = mix * head_mask
        mean = jnp.sum(mix * mix, axis=-1, keepdims=True) / pair
        return mix * lax.rsqrt(mean + EPS) * gain_row

    for w in range(waves):
        per_wave = ROWS // batch
        for k in range(per_wave):
            mix = attend(w * ROWS + k * batch)
            for h in range(heads_local):
                mixbuf[w * heads_local + h, k * ROWS : (k + 1) * ROWS, :] = mix[:, h * pair : (h + 1) * pair]
        heads = [
            mixbuf[w * heads_local + h, pl.ds(h, ROWS, stride=heads_local), :] for h in range(heads_local)
        ]
        heads = jnp.concatenate(heads, axis=1).astype(BF16)
        for d in [*range(1, n_tp), 0]:
            block = wo[:, pl.ds(pl.multiple_of(ot[d] * cols, cols), cols)]
            term = mm(heads, block).astype(BF16)
            if d:
                tsend[w, d] = term
                remote(tsend.at[w, d], trecv.at[w, d], t_sem.at[0, w], t_sem.at[1, w], ep, ot[d]).start()
            else:
                trecv[w, 0] = term

    rows_of = iota((ROWS, colsp), 0)
    resid = []
    parts = d_rs.shape[1]
    others = n_tp * n_ep
    for w in range(waves):
        slab_wait(trecv.at[w, 1:n_tp], t_sem.at[1, w])
        attn = trecv[w, 0].astype(F32)
        for d in range(1, n_tp):
            attn = attn + trecv[w, d].astype(F32)
        res = placed_tokens[w * ROWS : (w + 1) * ROWS] + attn
        resid.append(res)
        rows = res * gain_part
        for g in range(n_groups):
            if pack == 2:
                first = roll_rows(rows[:, :colsp], -g * hc)
                second = roll_rows(rows[:, colsp:], hc - g * hc)
                dsend[w, g] = jnp.where(rows_of < hc, first, second).astype(BF16)
            else:
                dsend[w, g] = roll_rows(rows, -g * hc).astype(BF16)
        squares = jnp.sum(res * res, axis=-1, keepdims=True)
        wide = jnp.where(iota((ROWS, 128), 0) == iota((ROWS, 128), 1), squares, 0.0)
        ssend[w] = jnp.sum(wide, axis=0, keepdims=True)
        for t in [*range(1, n_tp), 0]:
            for e in range(n_ep):
                if t or e:
                    at = t * n_ep + e
                    arrived = d_rs.at[w, t * parts // n_tp]
                    remote(dsend.at[w, oe[e] // EPG], drecv.at[w, at], d_ss.at[w], arrived, oe[e], ot[t]).start()
                    remote(ssend.at[w], srecv.at[w, at], s_sem.at[0, w], s_sem.at[1, w], oe[e], ot[t]).start()
        drecv[w, 0] = dsend[w, ep // EPG]
        srecv[w, 0] = ssend[w]

    rows32 = iota((slots, w_gate.shape[2]), 0) % ROWS
    for i in range(4, 7):
        weight_copies[i].wait()
    for w in range(waves):
        hid = w_gate.shape[2]
        gates = [jnp.zeros((slots, hid), F32) for _ in range(pack)]
        uppers = [jnp.zeros((slots, hid), F32) for _ in range(pack)]
        for t in range(n_tp):
            step = n_tp // parts
            if t % step == 0:
                slab_wait(drecv.at[w, max(t * n_ep, 1) : (t + step) * n_ep], d_rs.at[w, t // step])
            x = drecv[w, t * n_ep : (t + 1) * n_ep].reshape(slots, colsp)
            source = lax.rem(tp + n_tp - t, n_tp)
            for p in range(pack):
                at = pl.ds(pl.multiple_of(source * cols + p * colsp, colsp), colsp)
                gates[p] = gates[p] + mm(x, wg[0, at])
                uppers[p] = uppers[p] + mm(x, wu[0, at])
        slab_wait(srecv.at[w, 1:others], s_sem.at[1, w])
        squares = srecv[w, 0:n_ep]
        for t in range(1, n_tp):
            squares = squares + srecv[w, t * n_ep : (t + 1) * n_ep]
        squares = jnp.broadcast_to(squares, (n_ep, ROWS, 128)).reshape(slots, 128)
        slot = iota((slots, 128), 0) % ROWS
        if pack == 2:
            slot = slot % hc
        lane = (ep // EPG) * hc + slot
        lane = lax.rem(lane, ROWS)
        squares = jnp.sum(jnp.where(iota((slots, 128), 1) == lane, squares, 0.0), axis=-1, keepdims=True)
        inv = lax.rsqrt(squares / width + EPS)

        def join(parts):
            if pack == 1:
                return parts[0]
            down_shift = pltpu.roll(parts[1], slots - hc, 0)
            up_shift = pltpu.roll(parts[0], hc, 0)
            return jnp.where(rows32 < hc, parts[0] + down_shift, parts[1] + up_shift)

        gate = join(gates) * inv
        upper = join(uppers) * inv
        hidden = (gate / (1.0 + jnp.exp(-gate)) * upper).astype(BF16)
        for t in [*range(1, n_tp), 0]:
            downs = [
                mm(hidden, wd[0, :, pl.ds(pl.multiple_of(ot[t] * cols + p * colsp, colsp), colsp)]) for p in range(pack)
            ]
            down = downs[0] if pack == 1 else jnp.where(iota((slots, colsp), 0) % ROWS < hc, downs[0], downs[1])
            down = down.reshape(n_ep, ROWS, colsp).astype(BF16)
            csend[w, t * n_ep : (t + 1) * n_ep] = down
            for e in range(n_ep):
                if t or e:
                    at = t * n_ep + e
                    remote(csend.at[w, at], crecv.at[w, at], e_sem.at[0, w], e_sem.at[1, w], back[e], ot[t]).start()
        crecv[w, 0] = csend[w, 0]

    slab_wait(nsend.at[1:n_ep], n_sem.at[0])
    slab_wait(qpart.at[1:n_ep], p_sem.at[0])
    slab_wait(kvpart.at[1:n_ep], p_sem.at[2])
    for w in range(waves):
        slab_wait(tsend.at[w, 1:n_tp], t_sem.at[0, w])
        slab_wait(drecv.at[w, 1:others], d_ss.at[w])
        slab_wait(srecv.at[w, 1:others], s_sem.at[0, w])
        slab_wait(csend.at[w, 1:others], e_sem.at[0, w])

    final = None
    for w in range(waves):
        slab_wait(crecv.at[w, 1:others], e_sem.at[1, w])
        routed = [jnp.zeros((ROWS, colsp), F32) for _ in range(pack)]
        for g in range(n_groups):
            total = jnp.zeros((ROWS, colsp), F32)
            for m in range(EPG):
                e = lax.rem(g * EPG + m - ep + n_ep, n_ep)
                out = crecv[w, e].astype(F32)
                for t in range(1, n_tp):
                    out = out + crecv[w, t * n_ep + e].astype(F32)
                total = total + weights_of[w][g][m] * out.astype(BF16).astype(F32)
            for p in range(pack):
                routed[p] = jnp.where(rows_of // hc == g, roll_rows(total, g * hc - p * hc), routed[p])
        routed = routed[0] if pack == 1 else jnp.concatenate(routed, axis=1)
        placed = (resid[w] + routed).astype(BF16)
        part = mm(from_place[:, w * ROWS : (w + 1) * ROWS], placed)
        final = part if final is None else final + part
    mixed[...] = final.astype(BF16)


def finish_kernel(a, b, c, x, y, z):
    x[...] = a[...]
    y[...] = b[...]
    z[...] = c[...]


def on_device(
    tokens, attn_gain, w_query, w_key, w_value, mix_lambda, head_gain, w_output, cache_keys, cache_value,
    lengths, moe_gain, group_ids, member_ids, group_gate, member_logits, w_exp_gate, w_exp_up, w_exp_down,
):
    n_ep, n_tp = lax.axis_size("ep"), lax.axis_size("tp")
    seqs, width = tokens.shape
    qk_cols = w_query.shape[1]
    heads_local = mix_lambda.shape[0]
    cols = width // n_tp
    waves = seqs // ROWS
    n_groups = n_ep // EPG
    hc = ROWS // n_groups
    pack = 2 if hc * 2 == ROWS and cols % 256 == 0 else 1
    colsp = cols // pack
    devices = n_ep * n_tp
    vmem = pl.BlockSpec(memory_space=pltpu.VMEM)
    hbm = pl.BlockSpec(memory_space=pl.ANY)
    dma = pltpu.SemaphoreType.DMA
    like = lambda a: pltpu.VMEM(a.shape, a.dtype)
    operands = (
        tokens, attn_gain[None, :], head_gain[None, :], moe_gain[None, :], mix_lambda, lengths, group_ids,
        group_ids[None, :], member_ids.T, group_gate[None, :], member_logits.T,
        w_query, w_key, w_value, cache_keys, cache_value, w_output, w_exp_gate, w_exp_up, w_exp_down,
    )
    held = [
        pltpu.SMEM(a.shape, a.dtype) if i in (4, 5, 6) else like(a) for i, a in enumerate(operands[:11])
    ]
    scratch = held + [
        like(w_query), like(w_key), like(w_value), like(cache_keys), like(cache_value),
        pltpu.VMEM((seqs, qk_cols, cache_keys.shape[1]), BF16),
        like(w_output), like(w_exp_gate), like(w_exp_up), like(w_exp_down),
        pltpu.VMEM((n_ep, seqs, width // n_ep), BF16),
        pltpu.VMEM((n_ep, seqs, width // n_ep), BF16),
        pltpu.VMEM((n_ep, seqs, qk_cols), F32),
        pltpu.VMEM((n_ep, seqs, 2 * qk_cols), BF16),
        pltpu.VMEM((n_ep, seqs, qk_cols), F32),
        pltpu.VMEM((n_ep, seqs, 2 * qk_cols), BF16),
        pltpu.VMEM((waves * heads_local, ROWS * heads_local, qk_cols // heads_local), F32),
        pltpu.VMEM((waves, n_tp, ROWS, cols), BF16),
        pltpu.VMEM((waves, n_tp, ROWS, cols), BF16),
        pltpu.VMEM((waves, n_groups, ROWS, colsp), BF16),
        pltpu.VMEM((waves, devices, ROWS, colsp), BF16),
        pltpu.VMEM((waves, 1, 128), F32),
        pltpu.VMEM((waves, devices, 1, 128), F32),
        pltpu.VMEM((waves, devices, ROWS, colsp), BF16),
        pltpu.VMEM((waves, devices, ROWS, colsp), BF16),
        dma((11,)), dma((7,)), dma((seqs // LOAD + 1,)), dma((2,)), dma((4,)), dma((2, waves)),
        dma((waves,)), dma((waves, 4)), dma((2, waves)), dma((2, waves)),
    ]
    shapes = (
        jax.ShapeDtypeStruct((seqs, cols), BF16),
        jax.ShapeDtypeStruct((seqs, qk_cols), BF16),
        jax.ShapeDtypeStruct((seqs, qk_cols), BF16),
    )
    results = pl.pallas_call(
        functools.partial(layer_kernel, n_ep, n_tp),
        out_shape=shapes,
        in_specs=[hbm] * len(operands),
        out_specs=(vmem, vmem, vmem),
        scratch_shapes=scratch,
        compiler_params=pltpu.CompilerParams(
            collective_id=0, has_side_effects=True, vmem_limit_bytes=60 * 1024 * 1024
        ),
        name="decode_layer",
    )(*operands)
    return pl.pallas_call(
        finish_kernel, out_shape=shapes, in_specs=[vmem] * 3, out_specs=(vmem,) * 3, name="finish"
    )(*results)


def solution(mesh):
    return jax.shard_map(
        on_device,
        mesh=mesh,
        in_specs=(
            P("ep", None),
            P(),
            P("ep", "tp"),
            P("ep", "tp"),
            P("ep", "tp"),
            P("tp"),
            P(),
            P("tp", None),
            P("ep", None, "tp"),
            P("ep", None, "tp"),
            P("ep"),
            P(),
            P("ep"),
            P("ep", None),
            P("ep"),
            P("ep", None),
            P("ep", None, "tp"),
            P("ep", None, "tp"),
            P("ep", "tp", None),
        ),
        out_specs=(P("ep", "tp"), P("ep", "tp"), P("ep", "tp")),
        check_vma=False,
    )
```

```python
import functools

import jax
import jax.numpy as jnp
from jax import lax
from jax.experimental import pallas as pl
from jax.experimental.pallas import tpu as pltpu
from jax.sharding import PartitionSpec as P

EPG = 2
EPS = 1e-06
MESH = pl.DeviceIdType.MESH
F32 = jnp.float32
BF16 = jnp.bfloat16
LOAD = 4
ROWS = 8
LANES = 128


def iota(shape, dim):
    return lax.broadcasted_iota(jnp.int32, shape, dim)


def roll_rows(x, shift):
    shift = shift % ROWS
    return pltpu.roll(x, shift, 0) if shift else x


def mm(a, b):
    return jnp.dot(a, b, preferred_element_type=F32)


def layer_kernel(
    n_ep, n_tp,
    tokens_h, attn_gain_h, head_gain_h, moe_gain_h, lam_h, lengths_h, groups_h, groups_row_h, members_h, gate_h, logits_h,
    w_query, w_key, w_value, cache_keys, cache_value, w_output, w_gate, w_up, w_down,
    mixed, fresh_keys, fresh_value,
    tokens, attn_gain, head_gain, moe_gain, lam, lengths, groups, groups_row, members, group_gate, logits,
    wq, wk, wv, kbuf, vbuf, ktrans, wo, wg, wu, wd,
    nsend, nrecv, qpart, kvpart, qprecv, kvprecv, mixbuf,
    tsend, trecv, dsend, drecv, ssend, srecv, spart, sother, csend, crecv,
    i_sem, w_sem, c_sem, n_sem, p_sem, t_sem, d_ss, d_rs, f_sem, s_sem, g_sem, e_sem, known,
):
    ep = lax.axis_index("ep")
    tp = lax.axis_index("tp")
    seqs, width = tokens.shape
    rows_local = width // n_ep
    qk_cols = w_query.shape[1]
    heads_local = lam.shape[0]
    pair = qk_cols // heads_local
    head_dim = pair // 2
    total_heads = heads_local * n_tp
    positions = cache_keys.shape[1]
    cols = width // n_tp
    waves = seqs // ROWS
    n_groups = n_ep // EPG
    hc = ROWS // n_groups
    colsp = dsend.shape[-1]
    pack = cols // colsp
    batch = ROWS // heads_local
    slots = n_ep * ROWS

    oe = [lax.rem(ep + d, n_ep) for d in range(n_ep)]
    ot = [lax.rem(tp + d, n_tp) for d in range(n_tp)]

    barrier = pltpu.get_barrier_semaphore()
    near = sorted({1, n_tp - 1})
    for d in near:
        pl.semaphore_signal(barrier, inc=1, device_id={"ep": ep, "tp": ot[d]}, device_id_type=MESH)
    for d in range(1, n_ep):
        pl.semaphore_signal(barrier, inc=1, device_id={"ep": oe[d], "tp": tp}, device_id_type=MESH)

    small = [
        (tokens_h, tokens), (attn_gain_h, attn_gain), (head_gain_h, head_gain), (moe_gain_h, moe_gain), (lam_h, lam),
        (lengths_h, lengths), (groups_h, groups), (groups_row_h, groups_row), (members_h, members),
        (gate_h, group_gate), (logits_h, logits),
    ]
    small_copies = [pltpu.make_async_copy(s, d, i_sem.at[i]) for i, (s, d) in enumerate(small)]
    for c in small_copies:
        c.start()
    weight_pairs = [
        (w_query, wq), (w_key, wk), (w_value, wv), (w_output, wo.at[:, :width]), (w_gate, wg), (w_up, wu),
        (w_down, wd.at[:, :, :width]),
    ]
    weight_copies = [pltpu.make_async_copy(s, d, w_sem.at[i]) for i, (s, d) in enumerate(weight_pairs)]

    def key_copy(g):
        rows = pl.ds(g * LOAD, LOAD)
        return pltpu.make_async_copy(cache_keys.at[rows], kbuf.at[rows], c_sem.at[g])

    value_copy = pltpu.make_async_copy(cache_value, vbuf, c_sem.at[seqs // LOAD])

    for i in range(3):
        weight_copies[i].start(priority=1)
    for g in range(seqs // LOAD):
        key_copy(g).start(priority=1)
    value_copy.start(priority=1)
    for i in range(3, 7):
        weight_copies[i].start(priority=1)

    small_copies[0].wait()
    small_copies[1].wait()
    resid_in = tokens[...].astype(F32)
    inv = lax.rsqrt(jnp.mean(resid_in * resid_in, axis=-1, keepdims=True) + EPS)
    normed = (resid_in * inv * attn_gain[...]).astype(BF16)
    for e in range(n_ep):
        nsend[e] = normed[:, e * rows_local : (e + 1) * rows_local]

    def remote(src, dst, ss, rs, e, t):
        return pltpu.make_async_remote_copy(
            src_ref=src, dst_ref=dst, send_sem=ss, recv_sem=rs, device_id={"ep": e, "tp": t}, device_id_type=MESH
        )

    pl.semaphore_wait(barrier, n_ep - 1 + len(near))
    hops = [1 << k for k in range((n_tp // 2).bit_length() - 1)]

    def tell(k):
        for side in range(2):
            at = ot[hops[k] if side else n_tp - hops[k]]
            pl.semaphore_signal(known.at[k, side], inc=1, device_id={"ep": ep, "tp": at}, device_id_type=MESH)

    def hear(k):
        for side in range(2):
            pl.semaphore_wait(known.at[k, side], 1)

    def slab_wait(ref, sem):
        pltpu.make_async_copy(ref, ref, sem).wait()

    for d in range(1, n_ep):
        remote(nsend.at[oe[d]], nrecv.at[d], n_sem.at[0], n_sem.at[1], oe[d], tp).start()
    if hops:
        tell(0)
    nrecv[0] = nsend[ep]

    eye = (iota((qk_cols, qk_cols), 0) == iota((qk_cols, qk_cols), 1)).astype(BF16)

    def turn(s, carry):
        flipped = lax.dot_general(eye, kbuf[s], (((1,), (1,)), ((), ())), preferred_element_type=F32)
        ktrans[s, :, :positions] = flipped.astype(BF16)
        return carry

    def turn_group(g, carry):
        key_copy(g).wait()
        lax.fori_loop(g * LOAD, (g + 1) * LOAD, turn, 0)
        return carry

    half = seqs // LOAD // 2
    lax.fori_loop(0, half, turn_group, 0)

    for c in weight_copies[:3]:
        c.wait()
    slab_wait(nrecv.at[1:n_ep], n_sem.at[1])
    for k in range(len(hops) - 1):
        hear(k)
        tell(k + 1)
    rows_all = nrecv[...].reshape(n_ep * seqs, rows_local)
    for i, w in enumerate((wq, wk, wv)):
        part = mm(rows_all, w[...]).reshape(n_ep, seqs, qk_cols)
        if i == 0:
            qpart[...] = part
        else:
            kvpart[:, :, (i - 1) * qk_cols : i * qk_cols] = part.astype(BF16)
    back = [lax.rem(ep + n_ep - d, n_ep) for d in range(n_ep)]
    for d in range(1, n_ep):
        remote(qpart.at[d], qprecv.at[d], p_sem.at[0], p_sem.at[1], back[d], tp).start()
        remote(kvpart.at[d], kvprecv.at[d], p_sem.at[2], p_sem.at[3], back[d], tp).start()

    lax.fori_loop(half, seqs // LOAD, turn_group, 0)

    for c in small_copies[2:]:
        c.wait()
    same_index = iota((seqs, seqs), 0) == iota((seqs, seqs), 1)

    def column(row):
        return jnp.sum(jnp.where(same_index, row, 0.0), axis=1, keepdims=True)

    group_row = groups_row[...].astype(F32)
    group_col = column(group_row)
    earlier = (group_col == group_row) & (iota((seqs, seqs), 0) < iota((seqs, seqs), 1))
    rank_row = jnp.sum(earlier.astype(F32), axis=0, keepdims=True)
    wave_row = jnp.floor(rank_row / hc)
    place_row = wave_row * ROWS + group_row * hc + (rank_row - wave_row * hc)
    place_col = column(place_row)
    to_place = (place_row == iota((seqs, seqs), 0).astype(F32)).astype(BF16)
    from_place = (place_col == iota((seqs, seqs), 1).astype(F32)).astype(BF16)

    ranks = []
    group_of = [groups[s] for s in range(seqs)]
    for s in range(seqs):
        r = jnp.int32(0)
        for before in range(s):
            r = r + jnp.where(group_of[before] == group_of[s], 1, 0)
        ranks.append(r)
    places = [(ranks[s] // hc) * ROWS + group_of[s] * hc + ranks[s] % hc for s in range(seqs)]
    perm = []
    for p in range(seqs):
        at = jnp.int32(0)
        for s in range(seqs):
            at = at + jnp.where(places[s] == p, s, 0)
        perm.append(at)

    lg = logits[...]
    ex = jnp.exp(lg - jnp.max(lg, axis=0, keepdims=True))
    route_rows = ex / jnp.sum(ex, axis=0, keepdims=True) * group_gate[...]
    shares = []
    for m in range(EPG):
        hit = (members[...] == m).astype(F32)
        shares.append(jnp.sum(route_rows * hit, axis=0, keepdims=True))
    row_col = iota((ROWS, 1), 0)
    slot_col = row_col % hc if pack == 2 else row_col

    def share_col(w, g, m):
        wanted = (w * ROWS + g * hc + slot_col).astype(F32)
        return jnp.sum(jnp.where(place_row == wanted, shares[m], 0.0), axis=1, keepdims=True)

    weights_of = [
        [[share_col(w, g, m) for m in range(EPG)] for g in range(n_groups)] for w in range(waves)
    ]

    my_cols = pl.ds(pl.multiple_of(tp * cols, cols), cols)
    placed_tokens = mm(to_place, tokens[:, my_cols])
    gain_part = moe_gain[:, my_cols]

    scale = head_dim ** (-0.5)
    row16 = iota((2 * ROWS, qk_cols), 0)
    col16 = iota((2 * ROWS, qk_cols), 1)
    head16 = row16 % heads_local
    map_mask = ((col16 // pair == head16) & ((col16 // head_dim) % 2 == row16 // ROWS)).astype(F32)
    seq16 = (row16 % ROWS) // heads_local
    head8 = iota((ROWS, qk_cols), 0) % heads_local
    head_mask = (iota((ROWS, qk_cols), 1) // pair == head8).astype(F32)
    seq8 = iota((ROWS, qk_cols), 0) // heads_local
    row_id = iota((2 * ROWS, 1), 0)
    slopes = jnp.exp2(-8.0 * ((tp * heads_local + row_id % heads_local).astype(F32) + 1.0) / total_heads)
    lam_col = jnp.zeros((ROWS, 1), F32)
    for h in range(heads_local):
        lam_col = jnp.where(row_col % heads_local == h, lam[h], lam_col)
    gain_row = jnp.concatenate([head_gain[...]] * heads_local, axis=1)
    spots = iota((1, positions), 1)
    pick16 = (row_id % ROWS) // heads_local

    value_copy.wait()
    if hops:
        hear(len(hops) - 1)

    slab_wait(qprecv.at[1:n_ep], p_sem.at[1])
    slab_wait(kvprecv.at[1:n_ep], p_sem.at[3])
    query = qpart[0]
    fresh = kvpart[0].astype(F32)
    for d in range(1, n_ep):
        query = query + qprecv[d]
        fresh = fresh + kvprecv[d].astype(F32)
    fresh = fresh.astype(BF16)
    fresh_keys[...] = fresh[:, :qk_cols]
    fresh_value[...] = fresh[:, qk_cols:]
    projected = jnp.concatenate([query.astype(BF16), fresh], axis=1)

    weight_copies[3].wait()

    def score(base):
        wanted = (base + pick16).astype(F32)
        spread = mm((place_row == wanted).astype(BF16), projected)
        q16 = spread[:, :qk_cols] * map_mask
        lens = jnp.zeros((2 * ROWS, 1), jnp.int32)
        old = None
        for i in range(batch):
            at = perm[base + i]
            lens = jnp.where(pick16 == i, lengths[at], lens)
            own = jnp.where(seq16 == i, q16, 0.0).astype(BF16)
            part = mm(own, ktrans[at, :, :positions])
            old = part if old is None else old + part
        new = jnp.sum(q16 * spread[:, qk_cols : 2 * qk_cols], axis=-1, keepdims=True) * scale
        return old, new, lens, spread[:ROWS, 2 * qk_cols :]

    def weigh(old, new, lens, value):
        old = old * scale - slopes * (lens - spots).astype(F32)
        old = jnp.where(spots < lens, old, -jnp.inf)
        top = jnp.maximum(jnp.max(old, axis=-1, keepdims=True), new)
        old = jnp.exp(old - top)
        new = jnp.exp(new - top)
        recip = 1.0 / (jnp.sum(old, axis=-1, keepdims=True) + new)
        old = old * recip
        new = new * recip
        weights = (old[:ROWS] - lam_col * old[ROWS:]).astype(BF16)
        fresh_weight = (new[:ROWS] - lam_col * new[ROWS:]).astype(BF16).astype(F32)
        return weights, fresh_weight * value

    def combine(base, weights, mix):
        for i in range(batch):
            part = mm(weights, vbuf[perm[base + i]])
            mix = mix + jnp.where(seq8 == i, part, 0.0)
        mix = mix * head_mask
        mean = jnp.sum(mix * mix, axis=-1, keepdims=True) / pair
        return mix * lax.rsqrt(mean + EPS) * gain_row

    def project(w, mixes):
        for k, mix in enumerate(mixes):
            for h in range(heads_local):
                mixbuf[w * heads_local + h, k * ROWS : (k + 1) * ROWS, :] = mix[:, h * pair : (h + 1) * pair]
        heads = [
            mixbuf[w * heads_local + h, pl.ds(h, ROWS, stride=heads_local), :] for h in range(heads_local)
        ]
        heads = jnp.concatenate(heads, axis=1).astype(BF16)
        for d in [*range(1, n_tp), 0]:
            block = wo[:, pl.ds(pl.multiple_of(ot[d] * cols, cols), cols)]
            term = mm(heads, block).astype(BF16)
            if d:
                tsend[w, d] = term
            else:
                trecv[w, 0] = term
        for d in range(1, n_tp):
            remote(tsend.at[w, d], trecv.at[w, d], t_sem.at[0, w], t_sem.at[1, w], ep, ot[d]).start()

    per_wave = ROWS // batch
    steps = seqs // batch
    scores = {}
    ready = {}
    mixes = []

    def prepare(k):
        if k < steps and k not in scores:
            scores[k] = score(k * batch)

    prepare(0)
    for k in range(steps):
        prepare(k + 1)
        ready[k] = weigh(*scores[k])
        if k % per_wave == per_wave - 1:
            prepare(k + 1)
        mixes.append(combine(k * batch, *ready[k]))
        if k % per_wave == per_wave - 1:
            project(k // per_wave, mixes[-per_wave:])

    rows_of = iota((ROWS, colsp), 0)
    resid = []
    others = n_tp * n_ep
    cores = 2
    floors = n_tp // cores
    core = lax.rem(tp, cores)
    floor = tp // cores
    sibling = tp + 1 - 2 * core
    half_slots = floors * n_ep
    up = [lax.rem(floor + d, floors) * cores + core for d in range(floors)]
    down_floor = [lax.rem(floor + floors - d, floors) * cores for d in range(floors)]
    far_first = sorted(range(1, floors), key=lambda d: (-min(d, floors - d), d)) + [0]
    near_first = far_first[::-1]
    for w in range(waves):
        slab_wait(trecv.at[w, 1:n_tp], t_sem.at[1, w])
        attn = trecv[w, 0].astype(F32)
        for d in range(1, n_tp):
            attn = attn + trecv[w, d].astype(F32)
        res = placed_tokens[w * ROWS : (w + 1) * ROWS] + attn
        resid.append(res)
        rows = res * gain_part
        for g in range(n_groups):
            if pack == 2:
                first = roll_rows(rows[:, :colsp], -g * hc)
                second = roll_rows(rows[:, colsp:], hc - g * hc)
                dsend[w, g] = jnp.where(rows_of < hc, first, second).astype(BF16)
            else:
                dsend[w, g] = roll_rows(rows, -g * hc).astype(BF16)
        squares = jnp.sum(res * res, axis=-1, keepdims=True)
        wide = jnp.where(iota((ROWS, 128), 0) == iota((ROWS, 128), 1), squares, 0.0)
        ssend[w] = jnp.sum(wide, axis=0, keepdims=True)
        for d in far_first:
            for e in range(n_ep):
                if d or e:
                    at = d * n_ep + e
                    remote(dsend.at[w, oe[e] // EPG], drecv.at[w, at], d_ss.at[w], d_rs.at[w, d], oe[e], up[d]).start()
                    remote(ssend.at[w], srecv.at[w, at], s_sem.at[0, w], s_sem.at[1, w], oe[e], up[d]).start()
        drecv[w, 0] = dsend[w, ep // EPG]
        srecv[w, 0] = ssend[w]

    rows32 = iota((slots, w_gate.shape[2]), 0) % ROWS
    for i in range(4, 7):
        weight_copies[i].wait()
    for w in range(waves):
        hid = w_gate.shape[2]
        gates = [jnp.zeros((slots, hid), F32) for _ in range(pack)]
        uppers = [jnp.zeros((slots, hid), F32) for _ in range(pack)]
        def feed(slot, source):
            x = drecv[w, slot * n_ep : (slot + 1) * n_ep].reshape(slots, colsp)
            for p in range(pack):
                at = pl.ds(pl.multiple_of(source * cols + p * colsp, colsp), colsp)
                gates[p] = gates[p] + mm(x, wg[0, at])
                uppers[p] = uppers[p] + mm(x, wu[0, at])

        for d in near_first:
            slab_wait(drecv.at[w, max(d * n_ep, 1) : (d + 1) * n_ep], d_rs.at[w, d])
            remote(
                drecv.at[w, d * n_ep : (d + 1) * n_ep], drecv.at[w, half_slots + d * n_ep : half_slots + (d + 1) * n_ep],
                f_sem.at[0, w], f_sem.at[1, w], ep, sibling,
            ).start()
        slab_wait(srecv.at[w, 1:half_slots], s_sem.at[1, w])
        squares = srecv[w, 0:n_ep]
        for d in range(1, floors):
            squares = squares + srecv[w, d * n_ep : (d + 1) * n_ep]
        spart[w] = squares
        remote(spart.at[w], sother.at[w], g_sem.at[0, w], g_sem.at[1, w], ep, sibling).start()
        for d in near_first:
            feed(d, down_floor[d] + core)
        slab_wait(drecv.at[w, half_slots:], f_sem.at[1, w])
        for d in near_first:
            feed(floors + d, down_floor[d] + 1 - core)
        slab_wait(sother.at[w], g_sem.at[1, w])
        squares = squares + sother[w]
        squares = jnp.broadcast_to(squares, (n_ep, ROWS, 128)).reshape(slots, 128)
        slot = iota((slots, 128), 0) % ROWS
        if pack == 2:
            slot = slot % hc
        lane = (ep // EPG) * hc + slot
        lane = lax.rem(lane, ROWS)
        squares = jnp.sum(jnp.where(iota((slots, 128), 1) == lane, squares, 0.0), axis=-1, keepdims=True)
        inv = lax.rsqrt(squares / width + EPS)

        def join(parts):
            if pack == 1:
                return parts[0]
            down_shift = pltpu.roll(parts[1], slots - hc, 0)
            up_shift = pltpu.roll(parts[0], hc, 0)
            return jnp.where(rows32 < hc, parts[0] + down_shift, parts[1] + up_shift)

        gate = join(gates) * inv
        upper = join(uppers) * inv
        hidden = (gate / (1.0 + jnp.exp(-gate)) * upper).astype(BF16)
        for t in [*range(1, n_tp), 0]:
            downs = [
                mm(hidden, wd[0, :, pl.ds(pl.multiple_of(ot[t] * cols + p * colsp, colsp), colsp)]) for p in range(pack)
            ]
            down = downs[0] if pack == 1 else jnp.where(iota((slots, colsp), 0) % ROWS < hc, downs[0], downs[1])
            down = down.reshape(n_ep, ROWS, colsp).astype(BF16)
            csend[w, t * n_ep : (t + 1) * n_ep] = down
        for t in [*range(1, n_tp), 0]:
            for e in range(n_ep):
                if t or e:
                    at = t * n_ep + e
                    remote(csend.at[w, at], crecv.at[w, at], e_sem.at[0, w], e_sem.at[1, w], back[e], ot[t]).start()
        crecv[w, 0] = csend[w, 0]

    slab_wait(nsend.at[1:n_ep], n_sem.at[0])
    slab_wait(qpart.at[1:n_ep], p_sem.at[0])
    slab_wait(kvpart.at[1:n_ep], p_sem.at[2])
    for w in range(waves):
        slab_wait(tsend.at[w, 1:n_tp], t_sem.at[0, w])
        slab_wait(drecv.at[w, 1:half_slots], d_ss.at[w])
        slab_wait(drecv.at[w, half_slots:], f_sem.at[0, w])
        slab_wait(srecv.at[w, 1:half_slots], s_sem.at[0, w])
        slab_wait(spart.at[w], g_sem.at[0, w])
        slab_wait(csend.at[w, 1:others], e_sem.at[0, w])

    final = None
    for w in range(waves):
        slab_wait(crecv.at[w, 1:others], e_sem.at[1, w])
        routed = [jnp.zeros((ROWS, colsp), F32) for _ in range(pack)]
        for g in range(n_groups):
            total = jnp.zeros((ROWS, colsp), F32)
            for m in range(EPG):
                e = lax.rem(g * EPG + m - ep + n_ep, n_ep)
                out = crecv[w, e].astype(F32)
                for t in range(1, n_tp):
                    out = out + crecv[w, t * n_ep + e].astype(F32)
                total = total + weights_of[w][g][m] * out.astype(BF16).astype(F32)
            for p in range(pack):
                routed[p] = jnp.where(rows_of // hc == g, roll_rows(total, g * hc - p * hc), routed[p])
        routed = routed[0] if pack == 1 else jnp.concatenate(routed, axis=1)
        placed = (resid[w] + routed).astype(BF16)
        part = mm(from_place[:, w * ROWS : (w + 1) * ROWS], placed)
        final = part if final is None else final + part
    mixed[...] = final.astype(BF16)


def finish_kernel(a, b, c, x, y, z):
    x[...] = a[...]
    y[...] = b[...]
    z[...] = c[...]


def on_device(
    tokens, attn_gain, w_query, w_key, w_value, mix_lambda, head_gain, w_output, cache_keys, cache_value,
    lengths, moe_gain, group_ids, member_ids, group_gate, member_logits, w_exp_gate, w_exp_up, w_exp_down,
):
    n_ep, n_tp = lax.axis_size("ep"), lax.axis_size("tp")
    seqs, width = tokens.shape
    qk_cols = w_query.shape[1]
    heads_local = mix_lambda.shape[0]
    cols = width // n_tp
    waves = seqs // ROWS
    n_groups = n_ep // EPG
    hc = ROWS // n_groups
    pack = 2 if hc * 2 == ROWS and cols % 256 == 0 else 1
    colsp = cols // pack
    devices = n_ep * n_tp
    vmem = pl.BlockSpec(memory_space=pltpu.VMEM)
    hbm = pl.BlockSpec(memory_space=pl.ANY)
    dma = pltpu.SemaphoreType.DMA
    like = lambda a: pltpu.VMEM(a.shape, a.dtype)
    padded = lambda a: pltpu.VMEM((*a.shape[:-1], a.shape[-1] + LANES), a.dtype)
    operands = (
        tokens, attn_gain[None, :], head_gain[None, :], moe_gain[None, :], mix_lambda, lengths, group_ids,
        group_ids[None, :], member_ids.T, group_gate[None, :], member_logits.T,
        w_query, w_key, w_value, cache_keys, cache_value, w_output, w_exp_gate, w_exp_up, w_exp_down,
    )
    held = [
        pltpu.SMEM(a.shape, a.dtype) if i in (4, 5, 6) else like(a) for i, a in enumerate(operands[:11])
    ]
    scratch = held + [
        like(w_query), like(w_key), like(w_value), like(cache_keys), like(cache_value),
        pltpu.VMEM((seqs, qk_cols, cache_keys.shape[1] + LANES), BF16),
        padded(w_output), like(w_exp_gate), like(w_exp_up), padded(w_exp_down),
        pltpu.VMEM((n_ep, seqs, width // n_ep), BF16),
        pltpu.VMEM((n_ep, seqs, width // n_ep), BF16),
        pltpu.VMEM((n_ep, seqs, qk_cols), F32),
        pltpu.VMEM((n_ep, seqs, 2 * qk_cols), BF16),
        pltpu.VMEM((n_ep, seqs, qk_cols), F32),
        pltpu.VMEM((n_ep, seqs, 2 * qk_cols), BF16),
        pltpu.VMEM((waves * heads_local, ROWS * heads_local, qk_cols // heads_local), F32),
        pltpu.VMEM((waves, n_tp, ROWS, cols), BF16),
        pltpu.VMEM((waves, n_tp, ROWS, cols), BF16),
        pltpu.VMEM((waves, n_groups, ROWS, colsp), BF16),
        pltpu.VMEM((waves, devices, ROWS, colsp), BF16),
        pltpu.VMEM((waves, 1, 128), F32),
        pltpu.VMEM((waves, devices // 2, 1, 128), F32),
        pltpu.VMEM((waves, n_ep, 1, 128), F32),
        pltpu.VMEM((waves, n_ep, 1, 128), F32),
        pltpu.VMEM((waves, devices, ROWS, colsp), BF16),
        pltpu.VMEM((waves, devices, ROWS, colsp), BF16),
        dma((11,)), dma((7,)), dma((seqs // LOAD + 1,)), dma((2,)), dma((4,)), dma((2, waves)),
        dma((waves,)), dma((waves, n_tp // 2)), dma((2, waves)), dma((2, waves)), dma((2, waves)), dma((2, waves)),
        pltpu.SemaphoreType.REGULAR((max((n_tp // 2).bit_length() - 1, 1), 2)),
    ]
    shapes = (
        jax.ShapeDtypeStruct((seqs, cols), BF16),
        jax.ShapeDtypeStruct((seqs, qk_cols), BF16),
        jax.ShapeDtypeStruct((seqs, qk_cols), BF16),
    )
    results = pl.pallas_call(
        functools.partial(layer_kernel, n_ep, n_tp),
        out_shape=shapes,
        in_specs=[hbm] * len(operands),
        out_specs=(vmem, vmem, vmem),
        scratch_shapes=scratch,
        compiler_params=pltpu.CompilerParams(
            collective_id=0, has_side_effects=True, vmem_limit_bytes=60 * 1024 * 1024
        ),
        name="decode_layer",
    )(*operands)
    return pl.pallas_call(
        finish_kernel, out_shape=shapes, in_specs=[vmem] * 3, out_specs=(vmem,) * 3, name="finish"
    )(*results)


def solution(mesh):
    return jax.shard_map(
        on_device,
        mesh=mesh,
        in_specs=(
            P("ep", None),
            P(),
            P("ep", "tp"),
            P("ep", "tp"),
            P("ep", "tp"),
            P("tp"),
            P(),
            P("tp", None),
            P("ep", None, "tp"),
            P("ep", None, "tp"),
            P("ep"),
            P(),
            P("ep"),
            P("ep", None),
            P("ep"),
            P("ep", None),
            P("ep", None, "tp"),
            P("ep", None, "tp"),
            P("ep", "tp", None),
        ),
        out_specs=(P("ep", "tp"), P("ep", "tp"), P("ep", "tp")),
        check_vma=False,
    )
```

```python
import functools

import jax
import jax.numpy as jnp
from jax import lax
from jax.experimental import pallas as pl
from jax.experimental.pallas import tpu as pltpu
from jax.sharding import PartitionSpec as P

EPG = 2
EPS = 1e-06
MESH = pl.DeviceIdType.MESH
F32 = jnp.float32
BF16 = jnp.bfloat16
LOAD = 4
ROWS = 8
LANES = 128


def iota(shape, dim):
    return lax.broadcasted_iota(jnp.int32, shape, dim)


def roll_rows(x, shift):
    shift = shift % ROWS
    return pltpu.roll(x, shift, 0) if shift else x


def mm(a, b):
    return jnp.dot(a, b, preferred_element_type=F32)


def layer_kernel(
    n_ep, n_tp,
    tokens_h, attn_gain_h, head_gain_h, moe_gain_h, lam_h, lengths_h, groups_h, groups_row_h, members_h, gate_h, logits_h,
    w_query, w_key, w_value, cache_keys, cache_value, w_output, w_gate, w_up, w_down,
    mixed, fresh_keys, fresh_value,
    tokens, attn_gain, head_gain, moe_gain, lam, lengths, groups, groups_row, members, group_gate, logits,
    wq, wk, wv, kbuf, vbuf, ktrans, wo, wg, wu, wd,
    nsend, nrecv, qpart, kvpart, qprecv, kvprecv, mixbuf,
    tsend, trecv, dsend, drecv, ssend, srecv, spart, sother, csend, crecv,
    i_sem, w_sem, c_sem, n_sem, p_sem, t_sem, d_ss, d_rs, f_sem, s_sem, g_sem, e_sem, known,
):
    ep = lax.axis_index("ep")
    tp = lax.axis_index("tp")
    seqs, width = tokens.shape
    rows_local = width // n_ep
    qk_cols = w_query.shape[1]
    heads_local = lam.shape[0]
    pair = qk_cols // heads_local
    head_dim = pair // 2
    total_heads = heads_local * n_tp
    positions = cache_keys.shape[1]
    cols = width // n_tp
    waves = seqs // ROWS
    n_groups = n_ep // EPG
    hc = ROWS // n_groups
    colsp = dsend.shape[-1]
    pack = cols // colsp
    batch = ROWS // heads_local
    slots = n_ep * ROWS

    oe = [lax.rem(ep + d, n_ep) for d in range(n_ep)]
    ot = [lax.rem(tp + d, n_tp) for d in range(n_tp)]

    barrier = pltpu.get_barrier_semaphore()
    for d in range(1, n_ep):
        pl.semaphore_signal(barrier, inc=1, device_id={"ep": oe[d], "tp": tp}, device_id_type=MESH)
    near = sorted({1, n_tp - 1})
    for d in near:
        pl.semaphore_signal(barrier, inc=1, device_id={"ep": ep, "tp": ot[d]}, device_id_type=MESH)

    small = [
        (tokens_h, tokens), (attn_gain_h, attn_gain), (head_gain_h, head_gain), (moe_gain_h, moe_gain), (lam_h, lam),
        (lengths_h, lengths), (groups_h, groups), (groups_row_h, groups_row), (members_h, members),
        (gate_h, group_gate), (logits_h, logits),
    ]
    small_copies = [pltpu.make_async_copy(s, d, i_sem.at[i]) for i, (s, d) in enumerate(small)]
    for c in small_copies:
        c.start()
    weight_pairs = [
        (w_query, wq), (w_key, wk), (w_value, wv), (w_output, wo.at[:, :width]), (w_gate, wg), (w_up, wu),
        (w_down, wd.at[:, :, :width]),
    ]
    weight_copies = [pltpu.make_async_copy(s, d, w_sem.at[i]) for i, (s, d) in enumerate(weight_pairs)]

    def key_copy(g):
        rows = pl.ds(g * LOAD, LOAD)
        return pltpu.make_async_copy(cache_keys.at[rows], kbuf.at[rows], c_sem.at[g])

    value_copy = pltpu.make_async_copy(cache_value, vbuf, c_sem.at[seqs // LOAD])

    for i in range(3):
        weight_copies[i].start(priority=1)
    for g in range(seqs // LOAD):
        key_copy(g).start(priority=1)
    value_copy.start(priority=1)
    for i in range(3, 7):
        weight_copies[i].start(priority=1)

    small_copies[0].wait()
    small_copies[1].wait()
    resid_in = tokens[...].astype(F32)
    inv = lax.rsqrt(jnp.mean(resid_in * resid_in, axis=-1, keepdims=True) + EPS)
    normed = (resid_in * inv * attn_gain[...]).astype(BF16)
    for e in range(n_ep):
        nsend[e] = normed[:, e * rows_local : (e + 1) * rows_local]

    def remote(src, dst, ss, rs, e, t):
        return pltpu.make_async_remote_copy(
            src_ref=src, dst_ref=dst, send_sem=ss, recv_sem=rs, device_id={"ep": e, "tp": t}, device_id_type=MESH
        )

    pl.semaphore_wait(barrier, n_ep - 1 + len(near))
    hops = [1 << k for k in range((n_tp // 2).bit_length() - 1)]

    def tell(k):
        for side in range(2):
            at = ot[hops[k] if side else n_tp - hops[k]]
            pl.semaphore_signal(known.at[k, side], inc=1, device_id={"ep": ep, "tp": at}, device_id_type=MESH)

    def hear(k):
        for side in range(2):
            pl.semaphore_wait(known.at[k, side], 1)

    def slab_wait(ref, sem):
        pltpu.make_async_copy(ref, ref, sem).wait()

    for d in range(1, n_ep):
        remote(nsend.at[oe[d]], nrecv.at[d], n_sem.at[0], n_sem.at[1], oe[d], tp).start()
    if hops:
        tell(0)
    nrecv[0] = nsend[ep]

    eye = (iota((qk_cols, qk_cols), 0) == iota((qk_cols, qk_cols), 1)).astype(BF16)

    def turn(s, carry):
        flipped = lax.dot_general(eye, kbuf[s], (((1,), (1,)), ((), ())), preferred_element_type=F32)
        ktrans[s, :, :positions] = flipped.astype(BF16)
        return carry

    def turn_group(g, carry):
        key_copy(g).wait()
        lax.fori_loop(g * LOAD, (g + 1) * LOAD, turn, 0)
        return carry

    half = seqs // LOAD // 2
    lax.fori_loop(0, half, turn_group, 0)

    for c in weight_copies[:3]:
        c.wait()
    slab_wait(nrecv.at[1:n_ep], n_sem.at[1])
    rows_all = nrecv[...].reshape(n_ep * seqs, rows_local)
    for i, w in enumerate((wq, wk, wv)):
        part = mm(rows_all, w[...]).reshape(n_ep, seqs, qk_cols)
        if i == 0:
            qpart[...] = part
        else:
            kvpart[:, :, (i - 1) * qk_cols : i * qk_cols] = part.astype(BF16)
    back = [lax.rem(ep + n_ep - d, n_ep) for d in range(n_ep)]
    for d in range(1, n_ep):
        remote(qpart.at[d], qprecv.at[d], p_sem.at[0], p_sem.at[1], back[d], tp).start()
        remote(kvpart.at[d], kvprecv.at[d], p_sem.at[2], p_sem.at[3], back[d], tp).start()

    for k in range(len(hops) - 1):
        hear(k)
        tell(k + 1)
    lax.fori_loop(half, seqs // LOAD, turn_group, 0)

    for c in small_copies[2:]:
        c.wait()
    same_index = iota((seqs, seqs), 0) == iota((seqs, seqs), 1)

    def column(row):
        return jnp.sum(jnp.where(same_index, row, 0.0), axis=1, keepdims=True)

    group_row = groups_row[...].astype(F32)
    group_col = column(group_row)
    earlier = (group_col == group_row) & (iota((seqs, seqs), 0) < iota((seqs, seqs), 1))
    rank_row = jnp.sum(earlier.astype(F32), axis=0, keepdims=True)
    wave_row = jnp.floor(rank_row / hc)
    place_row = wave_row * ROWS + group_row * hc + (rank_row - wave_row * hc)
    place_col = column(place_row)
    to_place = (place_row == iota((seqs, seqs), 0).astype(F32)).astype(BF16)
    from_place = (place_col == iota((seqs, seqs), 1).astype(F32)).astype(BF16)

    ranks = []
    group_of = [groups[s] for s in range(seqs)]
    for s in range(seqs):
        r = jnp.int32(0)
        for before in range(s):
            r = r + jnp.where(group_of[before] == group_of[s], 1, 0)
        ranks.append(r)
    places = [(ranks[s] // hc) * ROWS + group_of[s] * hc + ranks[s] % hc for s in range(seqs)]
    perm = []
    for p in range(seqs):
        at = jnp.int32(0)
        for s in range(seqs):
            at = at + jnp.where(places[s] == p, s, 0)
        perm.append(at)

    lg = logits[...]
    ex = jnp.exp(lg - jnp.max(lg, axis=0, keepdims=True))
    route_rows = ex / jnp.sum(ex, axis=0, keepdims=True) * group_gate[...]
    shares = []
    for m in range(EPG):
        hit = (members[...] == m).astype(F32)
        shares.append(jnp.sum(route_rows * hit, axis=0, keepdims=True))
    row_col = iota((ROWS, 1), 0)
    slot_col = row_col % hc if pack == 2 else row_col

    def share_col(w, g, m):
        wanted = (w * ROWS + g * hc + slot_col).astype(F32)
        return jnp.sum(jnp.where(place_row == wanted, shares[m], 0.0), axis=1, keepdims=True)

    weights_of = [
        [[share_col(w, g, m) for m in range(EPG)] for g in range(n_groups)] for w in range(waves)
    ]

    my_cols = pl.ds(pl.multiple_of(tp * cols, cols), cols)
    placed_tokens = mm(to_place, tokens[:, my_cols])
    gain_part = moe_gain[:, my_cols]

    scale = head_dim ** (-0.5)
    row16 = iota((2 * ROWS, qk_cols), 0)
    col16 = iota((2 * ROWS, qk_cols), 1)
    head16 = row16 % heads_local
    map_mask = ((col16 // pair == head16) & ((col16 // head_dim) % 2 == row16 // ROWS)).astype(F32)
    seq16 = (row16 % ROWS) // heads_local
    head8 = iota((ROWS, qk_cols), 0) % heads_local
    head_mask = (iota((ROWS, qk_cols), 1) // pair == head8).astype(F32)
    seq8 = iota((ROWS, qk_cols), 0) // heads_local
    row_id = iota((2 * ROWS, 1), 0)
    slopes = jnp.exp2(-8.0 * ((tp * heads_local + row_id % heads_local).astype(F32) + 1.0) / total_heads)
    lam_col = jnp.zeros((ROWS, 1), F32)
    for h in range(heads_local):
        lam_col = jnp.where(row_col % heads_local == h, lam[h], lam_col)
    gain_row = jnp.concatenate([head_gain[...]] * heads_local, axis=1)
    spots = iota((1, positions), 1)
    pick16 = (row_id % ROWS) // heads_local

    value_copy.wait()
    if hops:
        hear(len(hops) - 1)

    slab_wait(qprecv.at[1:n_ep], p_sem.at[1])
    slab_wait(kvprecv.at[1:n_ep], p_sem.at[3])
    query = qpart[0]
    fresh = kvpart[0].astype(F32)
    for d in range(1, n_ep):
        query = query + qprecv[d]
        fresh = fresh + kvprecv[d].astype(F32)
    fresh = fresh.astype(BF16)
    fresh_keys[...] = fresh[:, :qk_cols]
    fresh_value[...] = fresh[:, qk_cols:]
    projected = jnp.concatenate([query.astype(BF16), fresh], axis=1)

    weight_copies[3].wait()

    row_all = iota((seqs // batch * 2 * ROWS, 1), 0)
    wanted = (row_all // (2 * ROWS)) * batch + (row_all % ROWS) // heads_local
    spread_all = mm((place_row == wanted.astype(F32)).astype(BF16), projected)

    def score(base):
        spread = spread_all[base // batch * 2 * ROWS : (base // batch + 1) * 2 * ROWS]
        q16 = spread[:, :qk_cols] * map_mask
        lens = jnp.zeros((2 * ROWS, 1), jnp.int32)
        old = None
        for i in range(batch):
            at = perm[base + i]
            lens = jnp.where(pick16 == i, lengths[at], lens)
            own = jnp.where(seq16 == i, q16, 0.0).astype(BF16)
            part = mm(own, ktrans[at, :, :positions])
            old = part if old is None else old + part
        new = jnp.sum(q16 * spread[:, qk_cols : 2 * qk_cols], axis=-1, keepdims=True) * scale
        return old, new, lens, spread[:ROWS, 2 * qk_cols :]

    def weigh(old, new, lens, value):
        old = old * scale - slopes * (lens - spots).astype(F32)
        old = jnp.where(spots < lens, old, -jnp.inf)
        top = jnp.maximum(jnp.max(old, axis=-1, keepdims=True), new)
        old = jnp.exp(old - top)
        new = jnp.exp(new - top)
        recip = 1.0 / (jnp.sum(old, axis=-1, keepdims=True) + new)
        old = old * recip
        new = new * recip
        weights = (old[:ROWS] - lam_col * old[ROWS:]).astype(BF16)
        fresh_weight = (new[:ROWS] - lam_col * new[ROWS:]).astype(BF16).astype(F32)
        return weights, fresh_weight * value

    def combine(base, weights, mix):
        for i in range(batch):
            part = mm(weights, vbuf[perm[base + i]])
            mix = mix + jnp.where(seq8 == i, part, 0.0)
        mix = mix * head_mask
        mean = jnp.sum(mix * mix, axis=-1, keepdims=True) / pair
        return mix * lax.rsqrt(mean + EPS) * gain_row

    def project(w, mixes):
        for k, mix in enumerate(mixes):
            for h in range(heads_local):
                mixbuf[w * heads_local + h, k * ROWS : (k + 1) * ROWS, :] = mix[:, h * pair : (h + 1) * pair]
        heads = [
            mixbuf[w * heads_local + h, pl.ds(h, ROWS, stride=heads_local), :] for h in range(heads_local)
        ]
        heads = jnp.concatenate(heads, axis=1).astype(BF16)
        for d in [*range(1, n_tp), 0]:
            block = wo[:, pl.ds(pl.multiple_of(ot[d] * cols, cols), cols)]
            term = mm(heads, block).astype(BF16)
            if d:
                tsend[w, d] = term
            else:
                trecv[w, 0] = term
        for d in range(1, n_tp):
            remote(tsend.at[w, d], trecv.at[w, d], t_sem.at[0, w], t_sem.at[1, w], ep, ot[d]).start()

    per_wave = ROWS // batch
    steps = seqs // batch
    scores = {}
    ready = {}
    mixes = []

    def prepare(k):
        if k < steps and k not in scores:
            scores[k] = score(k * batch)

    prepare(0)
    for k in range(steps):
        prepare(k + 1)
        ready[k] = weigh(*scores[k])
        if k % per_wave == per_wave - 1:
            prepare(k + 1)
        mixes.append(combine(k * batch, *ready[k]))
        if k % per_wave == per_wave - 1:
            project(k // per_wave, mixes[-per_wave:])

    rows_of = iota((ROWS, colsp), 0)
    resid = []
    others = n_tp * n_ep
    cores = 2
    floors = n_tp // cores
    core = lax.rem(tp, cores)
    floor = tp // cores
    sibling = tp + 1 - 2 * core
    half_slots = floors * n_ep
    up = [lax.rem(floor + d, floors) * cores + core for d in range(floors)]
    down_floor = [lax.rem(floor + floors - d, floors) * cores for d in range(floors)]
    far_first = sorted(range(1, floors), key=lambda d: (-min(d, floors - d), d)) + [0]
    near_first = far_first[::-1]
    for w in range(waves):
        slab_wait(trecv.at[w, 1:n_tp], t_sem.at[1, w])
        attn = trecv[w, 0].astype(F32)
        for d in range(1, n_tp):
            attn = attn + trecv[w, d].astype(F32)
        res = placed_tokens[w * ROWS : (w + 1) * ROWS] + attn
        resid.append(res)
        rows = res * gain_part
        for g in range(n_groups):
            if pack == 2:
                first = roll_rows(rows[:, :colsp], -g * hc)
                second = roll_rows(rows[:, colsp:], hc - g * hc)
                dsend[w, g] = jnp.where(rows_of < hc, first, second).astype(BF16)
            else:
                dsend[w, g] = roll_rows(rows, -g * hc).astype(BF16)
        squares = jnp.sum(res * res, axis=-1, keepdims=True)
        wide = jnp.where(iota((ROWS, 128), 0) == iota((ROWS, 128), 1), squares, 0.0)
        ssend[w] = jnp.sum(wide, axis=0, keepdims=True)
        for d in far_first:
            for e in range(n_ep):
                if d or e:
                    at = d * n_ep + e
                    remote(dsend.at[w, oe[e] // EPG], drecv.at[w, at], d_ss.at[w], d_rs.at[w, d], oe[e], up[d]).start()
                    remote(ssend.at[w], srecv.at[w, at], s_sem.at[0, w], s_sem.at[1, w], oe[e], up[d]).start()
        drecv[w, 0] = dsend[w, ep // EPG]
        srecv[w, 0] = ssend[w]

    rows32 = iota((slots, w_gate.shape[2]), 0) % ROWS
    for i in range(4, 7):
        weight_copies[i].wait()
    for w in range(waves):
        hid = w_gate.shape[2]
        gates = [jnp.zeros((slots, hid), F32) for _ in range(pack)]
        uppers = [jnp.zeros((slots, hid), F32) for _ in range(pack)]
        def feed(slot, source):
            x = drecv[w, slot * n_ep : (slot + 1) * n_ep].reshape(slots, colsp)
            for p in range(pack):
                at = pl.ds(pl.multiple_of(source * cols + p * colsp, colsp), colsp)
                gates[p] = gates[p] + mm(x, wg[0, at])
                uppers[p] = uppers[p] + mm(x, wu[0, at])

        for d in near_first:
            slab_wait(drecv.at[w, max(d * n_ep, 1) : (d + 1) * n_ep], d_rs.at[w, d])
            remote(
                drecv.at[w, d * n_ep : (d + 1) * n_ep], drecv.at[w, half_slots + d * n_ep : half_slots + (d + 1) * n_ep],
                f_sem.at[0, w], f_sem.at[1, w], ep, sibling,
            ).start()
        slab_wait(srecv.at[w, 1:half_slots], s_sem.at[1, w])
        squares = srecv[w, 0:n_ep]
        for d in range(1, floors):
            squares = squares + srecv[w, d * n_ep : (d + 1) * n_ep]
        spart[w] = squares
        remote(spart.at[w], sother.at[w], g_sem.at[0, w], g_sem.at[1, w], ep, sibling).start()
        for d in near_first:
            feed(d, down_floor[d] + core)
        slab_wait(drecv.at[w, half_slots:], f_sem.at[1, w])
        for d in near_first:
            feed(floors + d, down_floor[d] + 1 - core)
        slab_wait(sother.at[w], g_sem.at[1, w])
        squares = squares + sother[w]
        squares = jnp.broadcast_to(squares, (n_ep, ROWS, 128)).reshape(slots, 128)
        slot = iota((slots, 128), 0) % ROWS
        if pack == 2:
            slot = slot % hc
        lane = (ep // EPG) * hc + slot
        lane = lax.rem(lane, ROWS)
        squares = jnp.sum(jnp.where(iota((slots, 128), 1) == lane, squares, 0.0), axis=-1, keepdims=True)
        inv = lax.rsqrt(squares / width + EPS)

        def join(parts):
            if pack == 1:
                return parts[0]
            down_shift = pltpu.roll(parts[1], slots - hc, 0)
            up_shift = pltpu.roll(parts[0], hc, 0)
            return jnp.where(rows32 < hc, parts[0] + down_shift, parts[1] + up_shift)

        gate = join(gates) * inv
        upper = join(uppers) * inv
        hidden = (gate / (1.0 + jnp.exp(-gate)) * upper).astype(BF16)
        for t in [*range(1, n_tp), 0]:
            downs = [
                mm(hidden, wd[0, :, pl.ds(pl.multiple_of(ot[t] * cols + p * colsp, colsp), colsp)]) for p in range(pack)
            ]
            down = downs[0] if pack == 1 else jnp.where(iota((slots, colsp), 0) % ROWS < hc, downs[0], downs[1])
            down = down.reshape(n_ep, ROWS, colsp).astype(BF16)
            csend[w, t * n_ep : (t + 1) * n_ep] = down
        for t in [*range(1, n_tp), 0]:
            for e in range(n_ep):
                if t or e:
                    at = t * n_ep + e
                    remote(csend.at[w, at], crecv.at[w, at], e_sem.at[0, w], e_sem.at[1, w], back[e], ot[t]).start()
        crecv[w, 0] = csend[w, 0]

    slab_wait(nsend.at[1:n_ep], n_sem.at[0])
    slab_wait(qpart.at[1:n_ep], p_sem.at[0])
    slab_wait(kvpart.at[1:n_ep], p_sem.at[2])
    for w in range(waves):
        slab_wait(tsend.at[w, 1:n_tp], t_sem.at[0, w])
        slab_wait(drecv.at[w, 1:half_slots], d_ss.at[w])
        slab_wait(drecv.at[w, half_slots:], f_sem.at[0, w])
        slab_wait(srecv.at[w, 1:half_slots], s_sem.at[0, w])
        slab_wait(spart.at[w], g_sem.at[0, w])
        slab_wait(csend.at[w, 1:others], e_sem.at[0, w])

    final = None
    for w in range(waves):
        slab_wait(crecv.at[w, 1:others], e_sem.at[1, w])
        routed = [jnp.zeros((ROWS, colsp), F32) for _ in range(pack)]
        for g in range(n_groups):
            total = jnp.zeros((ROWS, colsp), F32)
            for m in range(EPG):
                e = lax.rem(g * EPG + m - ep + n_ep, n_ep)
                out = crecv[w, e].astype(F32)
                for t in range(1, n_tp):
                    out = out + crecv[w, t * n_ep + e].astype(F32)
                total = total + weights_of[w][g][m] * out.astype(BF16).astype(F32)
            for p in range(pack):
                routed[p] = jnp.where(rows_of // hc == g, roll_rows(total, g * hc - p * hc), routed[p])
        routed = routed[0] if pack == 1 else jnp.concatenate(routed, axis=1)
        placed = (resid[w] + routed).astype(BF16)
        part = mm(from_place[:, w * ROWS : (w + 1) * ROWS], placed)
        final = part if final is None else final + part
    mixed[...] = final.astype(BF16)


def finish_kernel(a, b, c, x, y, z):
    x[...] = a[...]
    y[...] = b[...]
    z[...] = c[...]


def on_device(
    tokens, attn_gain, w_query, w_key, w_value, mix_lambda, head_gain, w_output, cache_keys, cache_value,
    lengths, moe_gain, group_ids, member_ids, group_gate, member_logits, w_exp_gate, w_exp_up, w_exp_down,
):
    n_ep, n_tp = lax.axis_size("ep"), lax.axis_size("tp")
    seqs, width = tokens.shape
    qk_cols = w_query.shape[1]
    heads_local = mix_lambda.shape[0]
    cols = width // n_tp
    waves = seqs // ROWS
    n_groups = n_ep // EPG
    hc = ROWS // n_groups
    pack = 2 if hc * 2 == ROWS and cols % 256 == 0 else 1
    colsp = cols // pack
    devices = n_ep * n_tp
    vmem = pl.BlockSpec(memory_space=pltpu.VMEM)
    hbm = pl.BlockSpec(memory_space=pl.ANY)
    dma = pltpu.SemaphoreType.DMA
    like = lambda a: pltpu.VMEM(a.shape, a.dtype)
    padded = lambda a: pltpu.VMEM((*a.shape[:-1], a.shape[-1] + LANES), a.dtype)
    operands = (
        tokens, attn_gain[None, :], head_gain[None, :], moe_gain[None, :], mix_lambda, lengths, group_ids,
        group_ids[None, :], member_ids.T, group_gate[None, :], member_logits.T,
        w_query, w_key, w_value, cache_keys, cache_value, w_output, w_exp_gate, w_exp_up, w_exp_down,
    )
    held = [
        pltpu.SMEM(a.shape, a.dtype) if i in (4, 5, 6) else like(a) for i, a in enumerate(operands[:11])
    ]
    scratch = held + [
        like(w_query), like(w_key), like(w_value), like(cache_keys), like(cache_value),
        pltpu.VMEM((seqs, qk_cols, cache_keys.shape[1] + LANES), BF16),
        padded(w_output), like(w_exp_gate), like(w_exp_up), padded(w_exp_down),
        pltpu.VMEM((n_ep, seqs, width // n_ep), BF16),
        pltpu.VMEM((n_ep, seqs, width // n_ep), BF16),
        pltpu.VMEM((n_ep, seqs, qk_cols), F32),
        pltpu.VMEM((n_ep, seqs, 2 * qk_cols), BF16),
        pltpu.VMEM((n_ep, seqs, qk_cols), F32),
        pltpu.VMEM((n_ep, seqs, 2 * qk_cols), BF16),
        pltpu.VMEM((waves * heads_local, ROWS * heads_local, qk_cols // heads_local), F32),
        pltpu.VMEM((waves, n_tp, ROWS, cols), BF16),
        pltpu.VMEM((waves, n_tp, ROWS, cols), BF16),
        pltpu.VMEM((waves, n_groups, ROWS, colsp), BF16),
        pltpu.VMEM((waves, devices, ROWS, colsp), BF16),
        pltpu.VMEM((waves, 1, 128), F32),
        pltpu.VMEM((waves, devices // 2, 1, 128), F32),
        pltpu.VMEM((waves, n_ep, 1, 128), F32),
        pltpu.VMEM((waves, n_ep, 1, 128), F32),
        pltpu.VMEM((waves, devices, ROWS, colsp), BF16),
        pltpu.VMEM((waves, devices, ROWS, colsp), BF16),
        dma((11,)), dma((7,)), dma((seqs // LOAD + 1,)), dma((2,)), dma((4,)), dma((2, waves)),
        dma((waves,)), dma((waves, n_tp // 2)), dma((2, waves)), dma((2, waves)), dma((2, waves)), dma((2, waves)),
        pltpu.SemaphoreType.REGULAR((max((n_tp // 2).bit_length() - 1, 1), 2)),
    ]
    shapes = (
        jax.ShapeDtypeStruct((seqs, cols), BF16),
        jax.ShapeDtypeStruct((seqs, qk_cols), BF16),
        jax.ShapeDtypeStruct((seqs, qk_cols), BF16),
    )
    results = pl.pallas_call(
        functools.partial(layer_kernel, n_ep, n_tp),
        out_shape=shapes,
        in_specs=[hbm] * len(operands),
        out_specs=(vmem, vmem, vmem),
        scratch_shapes=scratch,
        compiler_params=pltpu.CompilerParams(
            collective_id=0, has_side_effects=True, vmem_limit_bytes=60 * 1024 * 1024
        ),
        name="decode_layer",
    )(*operands)
    return pl.pallas_call(
        finish_kernel, out_shape=shapes, in_specs=[vmem] * 3, out_specs=(vmem,) * 3, name="finish"
    )(*results)


def solution(mesh):
    return jax.shard_map(
        on_device,
        mesh=mesh,
        in_specs=(
            P("ep", None),
            P(),
            P("ep", "tp"),
            P("ep", "tp"),
            P("ep", "tp"),
            P("tp"),
            P(),
            P("tp", None),
            P("ep", None, "tp"),
            P("ep", None, "tp"),
            P("ep"),
            P(),
            P("ep"),
            P("ep", None),
            P("ep"),
            P("ep", None),
            P("ep", None, "tp"),
            P("ep", None, "tp"),
            P("ep", "tp", None),
        ),
        out_specs=(P("ep", "tp"), P("ep", "tp"), P("ep", "tp")),
        check_vma=False,
    )
```
